1024 devices in a mesh: sp: 256 (over z, y, core), tp: 4 (over x).
Axes of the slice: x: 4, y: 8, z: 16, core: 2. Of those that a mesh axis runs over, the one named last changes fastest.
Arguments:
- stream: bfloat16 [32768, 2048], P('sp', 'tp'), may hold values from -52 to 52
- norm_gain: float32 [2, 2048], replicated, may hold values from 0.1 to 1.9
- value_weight: bfloat16 [4096, 1024], P('sp', 'tp'), may hold values from -0.125 to 0.125
- gate_weight: bfloat16 [4096, 1024], P('sp', 'tp'), may hold values from -0.125 to 0.125
- conv_taps: float32 [2, 31, 1024], replicated, may hold values from -3 to 3
- ln_gain: float32 [2, 1024], replicated, may hold values from 0.1 to 1.9
- ln_bias: float32 [2, 1024], replicated, may hold values from -3 to 3
- out_weight: bfloat16 [1024, 4096], P('tp', 'sp'), may hold values from -0.1875 to 0.1875
- final_gain: float32 [2048], replicated, may hold values from 0.1 to 1.9
Outputs:
- result: bfloat16 [32768, 2048], P('sp', 'tp')
The draws below stay inside these ranges and needn't reach their ends.
All inputs are finite; a program needn't handle non-finite values.
Results may differ from the reference program's by a relative error of at most 0.014.
Values may be sent and summed in bfloat16 or wider, within the bound.
No kernel may reach another device: no remote copies, remote signals or barrier semaphores. Data moves between devices by JAX's collectives and lax.ppermute only.
A program may use at most 64 MiB of HBM per device.

```python
import math
import jax
import jax.numpy as jnp
from jax import lax

D = 2048
C = 1024
KW = 31
LAYERS = 2
TOKENS = 32768
N_TP = 4


def draw_stream(key, part):
    key_values, key_rows, key_cols = jax.random.split(key, 3)
    column_place = jnp.arange(D, dtype=jnp.float32) / D - 0.5
    col_scale = jnp.exp(jnp.log(8.0) * column_place + jax.random.uniform(key_cols, (D,), jnp.float32, -0.35, 0.35))
    row_scale = jnp.exp(jax.random.uniform(key_rows, (TOKENS, 1), jnp.float32, -1.15, 1.15))
    values = jnp.clip(jax.random.normal(key_values, (TOKENS, D), jnp.float32), -4.0, 4.0)
    return (values * row_scale * col_scale).astype(jnp.bfloat16)


def draw_conv_taps(key, part):
    key_values, key_chans = jax.random.split(key)
    chan_place = jnp.arange(C, dtype=jnp.float32) / C - 0.5
    chan_scale = jnp.exp(jnp.log(6.0) * chan_place + jax.random.uniform(key_chans, (C,), jnp.float32, -0.35, 0.35))
    values = jnp.clip(jax.random.normal(key_values, (LAYERS, KW, C), jnp.float32), -4.0, 4.0)
    return (values * chan_scale / math.sqrt(KW)).astype(jnp.float32)


def level_of(stream_key, shape, shards, smallest, high):
    factor_of = 1.0
    for dim, blocks in shards:
        draws = jax.random.uniform(jax.random.fold_in(jax.random.fold_in(stream_key, 6), dim), (blocks,), jnp.float32, smallest / len(shards), high / len(shards))
        factor_of = factor_of * jnp.repeat(jnp.exp(draws), shape[dim] // blocks).reshape((-1,) + (1,) * (len(shape) - 1 - dim))
    return factor_of


def gaussian(own_key, dims, deviation, most, shards=(), held_as=jnp.bfloat16):
    factor_of = level_of(own_key, dims, shards, -0.22, 0.18) if shards else 1.0
    result = jax.random.normal(own_key, dims, jnp.float32) * deviation * factor_of
    return jnp.minimum(jnp.maximum(result, -most), most).astype(held_as)


def setup_inputs(seed: int = 0) -> dict:
    arg_keys = jax.random.split(jax.random.key(seed), 10)
    stream = draw_stream(jax.random.fold_in(arg_keys[9], 71), 0)
    norm_gain = jnp.clip(1.0 + 0.18 * jax.random.normal(arg_keys[1], (LAYERS, D), jnp.float32), 0.1, 1.9)
    value_weight = gaussian(arg_keys[2], (LAYERS * D, C), D ** -0.5, 0.125, ((0, 256), (1, 4)))
    gate_weight = gaussian(arg_keys[3], (LAYERS * D, C), D ** -0.5, 0.125, ((0, 256), (1, 4)))
    conv_taps = draw_conv_taps(jax.random.fold_in(arg_keys[9], 71), 0)
    ln_gain = jnp.clip(1.0 + 0.18 * jax.random.normal(arg_keys[5], (LAYERS, C), jnp.float32), 0.1, 1.9)
    ln_bias = gaussian(arg_keys[6], (LAYERS, C), 0.5, 3.0, (), jnp.float32)
    out_weight = gaussian(arg_keys[7], (C, LAYERS * D), C ** -0.5, 0.1875, ((0, 4), (1, 256)))
    final_gain = jnp.clip(1.0 + 0.18 * jax.random.normal(arg_keys[8], (D,), jnp.float32), 0.1, 1.9)
    return {"stream": stream, "norm_gain": norm_gain, "value_weight": value_weight, "gate_weight": gate_weight, "conv_taps": conv_taps, "ln_gain": ln_gain, "ln_bias": ln_bias, "out_weight": out_weight, "final_gain": final_gain}


EPS = 1e-06

def valid_conv(extended, tap_table):
    length = extended.shape[0] - (KW - 1)
    running = tap_table[0] * extended[0:length]
    for tap_index in range(1, KW):
        running = running + tap_table[tap_index] * extended[tap_index:tap_index + length]
    return running

def reference(stream, norm_gain, value_weight, gate_weight, conv_taps, ln_gain, ln_bias, out_weight, final_gain):
    value_all = value_weight.reshape(D, LAYERS, C)
    gate_all = gate_weight.reshape(D, LAYERS, C)
    out_all = out_weight.reshape(C, D, LAYERS)
    block_width = C // N_TP
    current = stream
    for layer_index in range(LAYERS):
        current32 = current.astype(jnp.float32)
        scale = lax.rsqrt(lax.optimization_barrier(jnp.sum(current32 * current32, axis=1, keepdims=True)) / D + EPS)
        normed = (current32 * scale * norm_gain[layer_index]).astype(jnp.bfloat16)
        value_proj = jnp.dot(normed, value_all[:, layer_index], preferred_element_type=jnp.float32)
        gate_proj = jnp.dot(normed, gate_all[:, layer_index], preferred_element_type=jnp.float32)
        glu_out = value_proj * jax.nn.sigmoid(gate_proj)
        extended = jnp.concatenate([jnp.zeros((KW - 1, C), jnp.float32), glu_out], axis=0)
        conv_out = valid_conv(extended, conv_taps[layer_index])
        row_mean = lax.optimization_barrier(jnp.sum(conv_out, axis=1, keepdims=True)) / C
        row_var = lax.optimization_barrier(jnp.sum(conv_out * conv_out, axis=1, keepdims=True)) / C - row_mean * row_mean
        active = jax.nn.silu((conv_out - row_mean) * lax.rsqrt(row_var + EPS) * ln_gain[layer_index] + ln_bias[layer_index]).astype(jnp.bfloat16)
        branch = jnp.zeros((current.shape[0], D), jnp.float32)
        for block_index in range(N_TP):
            low = block_index * block_width
            partial_value = jnp.dot(active[:, low:low + block_width], out_all[low:low + block_width, :, layer_index], preferred_element_type=jnp.float32)
            branch = branch + lax.optimization_barrier(partial_value.astype(jnp.bfloat16)).astype(jnp.float32)
        current = (current32 + branch).astype(jnp.bfloat16)
    final32 = current.astype(jnp.float32)
    squares = lax.optimization_barrier(jnp.sum(final32 * final32, axis=1, keepdims=True))
    return (final32 * lax.rsqrt(squares / D + EPS) * final_gain).astype(jnp.bfloat16)
```

```python
import jax
import jax.numpy as jnp
from jax import lax
from jax.experimental import pallas as pl
from jax.experimental.pallas import tpu as pltpu
from jax.sharding import Mesh, PartitionSpec as P

KW = 31
LAYERS = 2
EPS = 1e-06
RIM = 32
VMEM = pl.BlockSpec(memory_space=pltpu.VMEM)
SMEM = pl.BlockSpec(memory_space=pltpu.SMEM)
F32 = jnp.float32
BF16 = jnp.bfloat16
INTERPRET = False


def call(body, out_shape, in_specs, scratch=(), flops=10**8, moved=10**6):
    return pl.pallas_call(
        body,
        out_shape=out_shape,
        in_specs=in_specs,
        out_specs=jax.tree.map(lambda _: VMEM, out_shape),
        scratch_shapes=list(scratch),
        cost_estimate=pl.CostEstimate(flops=flops, bytes_accessed=moved, transcendentals=0),
        compiler_params=pltpu.CompilerParams(vmem_limit_bytes=24 * 2**20),
        interpret=INTERPRET,
    )


def natural(mine, other, core):
    blocks = [jnp.where(core == 0, mine, other), jnp.where(core == 0, other, mine)]
    w = jnp.stack([jnp.swapaxes(b, 0, 1) for b in blocks], axis=2)
    return w.reshape(-1, w.shape[-1])


def first_half(info_ref, x_ref, gain_ref, w_ref, other_ref, taps_ref, out_ref, ext_ref):
    n_tp, rows, columns = x_ref.shape
    channels = w_ref.shape[-1]
    zs = w_ref.shape[1] // n_tp
    core = info_ref[1]
    out_rows = out_ref.shape[0]
    squares = jnp.zeros((rows, 1), F32)
    for t in range(n_tp):
        x = x_ref[t].astype(F32)
        squares = squares + jnp.sum(x * x, axis=1, keepdims=True)
    scale = lax.rsqrt(squares / (n_tp * columns) + EPS)
    value = jnp.zeros((rows, channels), F32)
    gate = jnp.zeros((rows, channels), F32)
    for t in range(n_tp):
        gain = gain_ref[:, t * columns : (t + 1) * columns]
        normed = (x_ref[t].astype(F32) * scale * gain).astype(BF16)
        span = slice(t * zs, (t + 1) * zs)
        value_w = natural(w_ref[:, span, 0], other_ref[:, span, 0], core)
        gate_w = natural(w_ref[:, span, 1], other_ref[:, span, 1], core)
        value = value + jnp.dot(normed, value_w, preferred_element_type=F32)
        gate = gate + jnp.dot(normed, gate_w, preferred_element_type=F32)
    glu = value * jax.nn.sigmoid(gate)
    row = lax.broadcasted_iota(jnp.int32, glu.shape, 0)
    ext_ref[...] = jnp.where(row >= info_ref[0], glu, 0.0)
    lead = RIM - (KW - 1)
    lanes = min(channels, 128)
    for low in range(0, channels, lanes):
        cols = slice(low, low + lanes)
        total = jnp.zeros((out_rows, lanes), F32)
        for s in range(8):
            last = (KW - 1 - s) // 8
            shifted = ext_ref[lead + s : lead + s + out_rows + 8 * last, cols]
            for j in range(last + 1):
                k = 8 * j + s
                total = total + taps_ref[k : k + 1, cols] * shifted[8 * j : 8 * j + out_rows]
        out_ref[:, cols] = total.astype(BF16)


def second_half(info_ref, c_ref, gain_ref, bias_ref, w_ref, other_ref, x_ref, out_ref):
    n_tp, rows, channels = c_ref.shape
    total_channels = n_tp * channels
    first = jnp.zeros((rows, 1), F32)
    second = jnp.zeros((rows, 1), F32)
    for t in range(n_tp):
        c = c_ref[t].astype(F32)
        first = first + jnp.sum(c, axis=1, keepdims=True)
        second = second + jnp.sum(c * c, axis=1, keepdims=True)
    mean = first / total_channels
    var = second / total_channels - mean * mean
    scale = lax.rsqrt(var + EPS)
    zs = w_ref.shape[1] // n_tp
    branch = jnp.zeros(x_ref.shape, F32)
    for t in range(n_tp):
        cols = slice(t * channels, (t + 1) * channels)
        v = (c_ref[t].astype(F32) - mean) * scale * gain_ref[:, cols] + bias_ref[:, cols]
        active = (v * jax.nn.sigmoid(v)).astype(BF16)
        span = slice(t * zs, (t + 1) * zs)
        w = natural(w_ref[:, span], other_ref[:, span], info_ref[1])
        part = lax.dot_general(active, w, (((1,), (1,)), ((), ())), preferred_element_type=F32)
        branch = branch + part.astype(BF16).astype(F32)
    out_ref[...] = (x_ref[...].astype(F32) + branch).astype(BF16)


def exchange(blocks, axis):
    return lax.all_to_all(blocks, axis, 0, 0, tiled=True)


def everyone(x, axis):
    return exchange(jnp.broadcast_to(x[None], (lax.axis_size(axis), *x.shape)), axis)


def local(stream, norm_gain, value_weight, gate_weight, conv_taps, ln_gain, ln_bias, out_weight, final_gain):
    nz, ny, nc, nt = (lax.axis_size(a) for a in ("z", "y", "core", "tp"))
    tokens, columns = stream.shape
    channels = value_weight.shape[1]
    depth = value_weight.shape[0] // LAYERS
    tp = lax.axis_index("tp")
    sp = (lax.axis_index("z") * ny + lax.axis_index("y")) * nc + lax.axis_index("core")

    def per_layer(w):
        return jnp.moveaxis(w.reshape(depth, LAYERS, channels), 1, 0)

    vg = jnp.stack([per_layer(value_weight), per_layer(gate_weight)], axis=1)
    out_t = per_layer(out_weight.T)
    zl = nz // nt
    pairs = []
    for z in range(nz):
        for t in range(nt):
            pairs.append((z * nt + t, ((t * zl) + z % zl) * nt + z // zl))

    out_t = lax.ppermute(out_t, ("z", "tp"), pairs)
    blocks = jnp.concatenate([vg[0], out_t[:1], vg[1], out_t[1:]], axis=0)
    along_z = everyone(blocks, "z")
    parts = [along_z[:, :2], along_z[:, 2], along_z[:, 3:5], along_z[:, 5]]
    gathered_w = []
    for part in parts:
        if gathered_w:
            part, gathered_w[-1] = lax.optimization_barrier((part, gathered_w[-1]))
        gathered_w.append(everyone(part, "y"))
    weights = [(w, lax.ppermute(w, "core", [(0, 1), (1, 0)])) for w in gathered_w]

    count = nz * ny * nc
    earlier = lax.ppermute(
        stream[-LAYERS * RIM :], ("z", "y", "core"), [(i, i + 1) for i in range(count - 1)]
    )
    current = jnp.concatenate([earlier, stream], axis=0)
    gathered = lax.all_gather(current, "tp")

    my_taps = lax.dynamic_slice_in_dim(conv_taps, tp * channels, channels, 2)
    my_final = lax.dynamic_slice_in_dim(final_gain, tp * columns, columns, 0)
    for layer in range(LAYERS):
        rows = tokens + (LAYERS - layer) * RIM
        out_rows = rows - RIM
        last = layer == LAYERS - 1
        info = jnp.stack([jnp.where(sp == 0, rows - tokens, 0), lax.axis_index("core")]).astype(jnp.int32)
        conv = call(
            first_half,
            jax.ShapeDtypeStruct((out_rows, channels), BF16),
            [SMEM] + [VMEM] * 5,
            [pltpu.VMEM((rows, channels), F32)],
            flops=4 * rows * columns * nt * channels,
        )(info, gathered, norm_gain[layer : layer + 1], *weights[2 * layer], my_taps[layer])
        conv = lax.all_gather(conv, "tp")
        out = weights[2 * layer + 1]
        current = call(
            second_half,
            jax.ShapeDtypeStruct((out_rows, columns), BF16),
            [SMEM] + [VMEM] * 6,
            flops=2 * out_rows * columns * nt * channels,
        )(info, conv, ln_gain[layer : layer + 1], ln_bias[layer : layer + 1], *out, current[RIM:])
        if not last:
            gathered = lax.all_gather(current, "tp")
    final32 = current.astype(F32)
    squares = lax.psum(jnp.sum(final32 * final32, axis=1), "tp")
    total = nt * columns
    return (final32 * lax.rsqrt(squares[:, None] / total + EPS) * my_final).astype(BF16)


def shape_of(mesh):
    n_sp, n_tp = mesh.devices.shape
    ny = {256: 8}.get(n_sp, 2)
    return n_sp // (2 * ny), ny, 2, n_tp


def solution(mesh):
    inner = Mesh(mesh.devices.reshape(shape_of(mesh)), ("z", "y", "core", "tp"))
    sp = ("z", "y", "core")
    placed = (P(sp, "tp"), P(), P(sp, "tp"), P(sp, "tp"), P(), P(), P(), P("tp", sp), P())
    return jax.shard_map(local, mesh=inner, in_specs=placed, out_specs=P(sp, "tp"), check_vma=False)
```

```python
import jax
import jax.numpy as jnp
from jax import lax
from jax.experimental import pallas as pl
from jax.experimental.pallas import tpu as pltpu
from jax.sharding import Mesh, PartitionSpec as P

KW = 31
LAYERS = 2
EPS = 1e-06
RIM = 32
LANES = 128
VMEM = pl.BlockSpec(memory_space=pltpu.VMEM)
SMEM = pl.BlockSpec(memory_space=pltpu.SMEM)
F32 = jnp.float32
BF16 = jnp.bfloat16
INTERPRET = False


def call(body, out_shape, n_in, scratch=(), flops=10**8):
    return pl.pallas_call(
        body,
        out_shape=out_shape,
        in_specs=[SMEM] + [VMEM] * n_in,
        out_specs=VMEM,
        scratch_shapes=list(scratch),
        cost_estimate=pl.CostEstimate(flops=flops, bytes_accessed=10**6, transcendentals=0),
        compiler_params=pltpu.CompilerParams(vmem_limit_bytes=20 * 2**20),
        interpret=INTERPRET,
    )


def weight_rows(refs, span, kind):
    here, *sides, far = refs
    ahead = [here] + [s.at[1] for s in sides] + [far] + [s.at[0] for s in reversed(sides)]
    blocks = [jnp.stack([b[core, span, kind] for core in range(2)], axis=1) for b in ahead]
    w = jnp.stack(blocks, axis=1)
    return w.reshape(-1, w.shape[-1])


def turned(x, shift):
    chunks = [
        pltpu.roll(x[:, low : low + LANES], shift, 1) for low in range(0, x.shape[1], LANES)
    ]
    return jnp.concatenate(chunks, axis=1)


def first_half(n_x, n_w, kinds, info_ref, *refs):
    x_refs, refs = refs[:n_x], refs[n_x:]
    w_refs, (gain_ref, taps_ref, out_ref, ext_ref) = refs[:n_w], refs[n_w:]
    n_tp, _, columns = x_refs[0].shape
    rows, channels = ext_ref.shape
    zs = w_refs[0].shape[1] // n_tp
    copies, out_rows = out_ref.shape[0], out_ref.shape[-2]
    blocks = [jnp.concatenate([r[t] for r in x_refs], axis=0).astype(F32) for t in range(n_tp)]
    squares = sum(jnp.sum(x * x, axis=1, keepdims=True) for x in blocks)
    scale = lax.rsqrt(squares / (n_tp * columns) + EPS)
    value = jnp.zeros((rows, channels), F32)
    gate = jnp.zeros((rows, channels), F32)
    for t in range(n_tp):
        gain = gain_ref[:, t * columns : (t + 1) * columns]
        normed = turned(blocks[t] * scale * gain, info_ref[1]).astype(BF16)
        span = slice(t * zs, (t + 1) * zs)
        value = value + jnp.dot(normed, weight_rows(w_refs, span, kinds[0]), preferred_element_type=F32)
        gate = gate + jnp.dot(normed, weight_rows(w_refs, span, kinds[1]), preferred_element_type=F32)
    glu = value * jax.nn.sigmoid(gate)
    row = lax.broadcasted_iota(jnp.int32, glu.shape, 0)
    ext_ref[...] = jnp.where(row >= info_ref[0], glu, 0.0)
    lead = RIM - (KW - 1)
    lanes = min(channels, LANES)
    for low in range(0, channels, lanes):
        cols = slice(low, low + lanes)
        total = jnp.zeros((out_rows, lanes), F32)
        for s in range(8):
            last = (KW - 1 - s) // 8
            shifted = ext_ref[lead + s : lead + s + out_rows + 8 * last, cols]
            for j in range(last + 1):
                k = 8 * j + s
                total = total + taps_ref[k : k + 1, cols] * shifted[8 * j : 8 * j + out_rows]
        if len(out_ref.shape) == 2:
            out_ref[:, cols] = total.astype(BF16)
        else:
            for copy in range(copies):
                out_ref[copy, :, cols] = total.astype(BF16)


def second_half(n_x, n_w, kind, info_ref, *refs):
    x_refs, refs = refs[:n_x], refs[n_x:]
    w_refs, (c_ref, gain_ref, bias_ref, out_ref) = refs[:n_w], refs[n_w:]
    n_tp, rows, channels = c_ref.shape
    total_channels = n_tp * channels
    blocks = [c_ref[t].astype(F32) for t in range(n_tp)]
    mean = sum(jnp.sum(c, axis=1, keepdims=True) for c in blocks) / total_channels
    square = sum(jnp.sum(c * c, axis=1, keepdims=True) for c in blocks) / total_channels
    scale = lax.rsqrt(square - mean * mean + EPS)
    zs = w_refs[0].shape[1] // n_tp
    branch = jnp.zeros((rows, out_ref.shape[-1]), F32)
    for t in range(n_tp):
        cols = slice(t * channels, (t + 1) * channels)
        v = (blocks[t] - mean) * scale * gain_ref[:, cols] + bias_ref[:, cols]
        active = (v * jax.nn.sigmoid(v)).astype(BF16)
        w = weight_rows(w_refs, slice(t * zs, (t + 1) * zs), kind)
        part = lax.dot_general(active, w, (((1,), (1,)), ((), ())), preferred_element_type=F32)
        branch = branch + part.astype(BF16).astype(F32)
    if n_x == 2:
        halo_ref, own_ref = x_refs
        x = jnp.concatenate([halo_ref[info_ref[3], RIM:], own_ref[...]], axis=0)
    else:
        x = x_refs[0][RIM:]
    result = (x.astype(F32) + turned(branch, info_ref[2])).astype(BF16)
    out_ref[...] = result


def everyone(x, axis):
    blocks = jnp.broadcast_to(x[None], (lax.axis_size(axis), *x.shape))
    return lax.all_to_all(blocks, axis, 0, 0, tiled=True)


def round_y(x, step=None):
    ny, nc = lax.axis_size("y"), lax.axis_size("core")
    pairs = [(y * nc + c, (y + 1 - 2 * c) % ny * nc + c) for y in range(ny) for c in range(nc)]
    here = lax.all_gather(x, "core")
    parts, moving = [here], here
    for _ in range(ny // 2 - 1):
        moving = lax.ppermute(moving, ("y", "core"), pairs)
        parts.append(lax.all_gather(moving, "core"))
    half = lax.dynamic_index_in_dim(moving, lax.axis_index("core"), 0, keepdims=False)
    parts.append(lax.all_gather(lax.ppermute(half, ("y", "core"), pairs), "core"))
    return parts


def local(stream, norm_gain, value_weight, gate_weight, conv_taps, ln_gain, ln_bias, out_weight, final_gain):
    nz, ny, nc, nt = (lax.axis_size(a) for a in ("z", "y", "core", "tp"))
    tokens, columns = stream.shape
    channels = value_weight.shape[1]
    depth = value_weight.shape[0] // LAYERS
    tp, y = lax.axis_index("tp"), lax.axis_index("y")
    sp = (lax.axis_index("z") * ny + y) * nc + lax.axis_index("core")

    def per_layer(w):
        return jnp.moveaxis(w.reshape(depth, LAYERS, channels), 1, 0)

    vg = jnp.stack([per_layer(value_weight), per_layer(gate_weight)], axis=1)
    first_z = everyone(vg[0], "z")
    zl = nz // nt
    pairs = [(z * nt + t, (t * zl + z % zl) * nt + z // zl) for z in range(nz) for t in range(nt)]
    out_t = lax.ppermute(per_layer(out_weight.T), ("z", "tp"), pairs)
    own = lax.all_gather(stream, "tp")
    count = nz * ny * nc
    halo = lax.ppermute(
        own[:, -LAYERS * RIM :], ("z", "y", "core"), [(i, i + 1) for i in range(count - 1)]
    )
    rest_z = everyone(jnp.concatenate([out_t[:1], vg[1], out_t[1:]], axis=0), "z")
    vg0 = round_y(first_z)
    out0 = round_y(rest_z[:, :1])
    vgo1 = round_y(rest_z[:, 1:])

    my_taps = lax.dynamic_slice_in_dim(conv_taps, tp * channels, channels, 2)
    my_final = lax.dynamic_slice_in_dim(final_gain, tp * columns, columns, 0)
    wide = 2 * depth
    first_w, second_w, kinds = (vg0, vgo1), (out0, vgo1), (0, 2)
    x_all, x_mine = (halo, own), (halo, stream)
    for layer in range(LAYERS):
        rows = tokens + (LAYERS - layer) * RIM
        out_rows = rows - RIM
        back = wide * y
        info = [jnp.where(sp == 0, rows - tokens, 0), jnp.where(y == 0, 0, wide * ny - back), back, tp]
        info = jnp.stack(info).astype(jnp.int32)
        w = first_w[layer]
        conv = call(
            lambda *refs: first_half(len(x_all), len(w), (0, 1), *refs),
            jax.ShapeDtypeStruct((out_rows, channels), BF16),
            len(x_all) + len(w) + 2,
            [pltpu.VMEM((rows, channels), F32)],
            flops=4 * rows * columns * nt * channels,
        )(info, *x_all, *w, norm_gain[layer : layer + 1], my_taps[layer])
        conv = lax.all_gather(conv, "tp")
        w = second_w[layer]
        mine = call(
            lambda *refs: second_half(len(x_mine), len(w), kinds[layer], *refs),
            jax.ShapeDtypeStruct((out_rows, columns), BF16),
            len(x_mine) + len(w) + 3,
            flops=2 * out_rows * columns * nt * channels,
        )(info, *x_mine, *w, conv, ln_gain[layer : layer + 1], ln_bias[layer : layer + 1])
        x_mine = (mine,)
        if layer < LAYERS - 1:
            x_all = (lax.all_gather(mine, "tp"),)
    final32 = mine.astype(F32)
    squares = lax.psum(jnp.sum(final32 * final32, axis=1), "tp")
    total = nt * columns
    return (final32 * lax.rsqrt(squares[:, None] / total + EPS) * my_final).astype(BF16)


def shape_of(mesh):
    n_sp, n_tp = mesh.devices.shape
    return n_sp // 16, 8, 2, n_tp


def solution(mesh):
    inner = Mesh(mesh.devices.reshape(shape_of(mesh)), ("z", "y", "core", "tp"))
    sp = ("z", "y", "core")
    placed = (P(sp, "tp"), P(), P(sp, "tp"), P(sp, "tp"), P(), P(), P(), P("tp", sp), P())
    return jax.shard_map(local, mesh=inner, in_specs=placed, out_specs=P(sp, "tp"), check_vma=False)
```

```python
import jax
import jax.numpy as jnp
from jax import lax
from jax.experimental import pallas as pl
from jax.experimental.pallas import tpu as pltpu
from jax.sharding import Mesh, PartitionSpec as P

KW = 31
LAYERS = 2
EPS = 1e-06
RIM = 32
LANES = 128
VMEM = pl.BlockSpec(memory_space=pltpu.VMEM)
SMEM = pl.BlockSpec(memory_space=pltpu.SMEM)
F32 = jnp.float32
BF16 = jnp.bfloat16
INTERPRET = False


def call(body, out_shape, n_in, scratch=(), flops=10**8):
    return pl.pallas_call(
        body,
        out_shape=out_shape,
        in_specs=[SMEM] + [VMEM] * n_in,
        out_specs=VMEM,
        scratch_shapes=list(scratch),
        cost_estimate=pl.CostEstimate(flops=flops, bytes_accessed=10**6, transcendentals=0),
        compiler_params=pltpu.CompilerParams(vmem_limit_bytes=20 * 2**20),
        interpret=INTERPRET,
    )


def weight_rows(refs, span, kind):
    here, *sides, far = refs
    ahead = [here] + [s.at[1] for s in sides] + [far] + [s.at[0] for s in reversed(sides)]
    blocks = [jnp.stack([b[core, span, kind] for core in range(2)], axis=1) for b in ahead]
    w = jnp.stack(blocks, axis=1)
    return w.reshape(-1, w.shape[-1])


def turned(x, shift):
    chunks = [
        pltpu.roll(x[:, low : low + LANES], shift, 1) for low in range(0, x.shape[1], LANES)
    ]
    return jnp.concatenate(chunks, axis=1)


def first_half(n_x, n_w, kinds, info_ref, *refs):
    x_refs, refs = refs[:n_x], refs[n_x:]
    w_refs, (gain_ref, taps_ref, out_ref, ext_ref) = refs[:n_w], refs[n_w:]
    n_tp, _, columns = gain_ref.shape
    rows, channels = ext_ref.shape
    zs = w_refs[0].shape[1] // n_tp
    out_rows = out_ref.shape[0]
    blocks = [(x_refs[t][...] if n_x > 1 else x_refs[0][t]).astype(F32) for t in range(n_tp)]
    squares = sum(jnp.sum(x * x, axis=1, keepdims=True) for x in blocks)
    scale = lax.rsqrt(squares / (n_tp * columns) + EPS)
    value = jnp.zeros((rows, channels), F32)
    gate = jnp.zeros((rows, channels), F32)
    for j in range(n_tp):
        t = info_ref[3 + j]
        normed = turned(blocks[j] * scale * gain_ref[t], info_ref[1]).astype(BF16)
        span = pl.ds(t * zs, zs)
        value = value + jnp.dot(normed, weight_rows(w_refs, span, kinds[0]), preferred_element_type=F32)
        gate = gate + jnp.dot(normed, weight_rows(w_refs, span, kinds[1]), preferred_element_type=F32)
    glu = value * jax.nn.sigmoid(gate)
    row = lax.broadcasted_iota(jnp.int32, glu.shape, 0)
    ext_ref[...] = jnp.where(row >= info_ref[0], glu, 0.0)
    lead = RIM - (KW - 1)
    lanes = min(channels, LANES)
    for low in range(0, channels, lanes):
        cols = slice(low, low + lanes)
        total = jnp.zeros((out_rows, lanes), F32)
        for s in range(8):
            last = (KW - 1 - s) // 8
            shifted = ext_ref[lead + s : lead + s + out_rows + 8 * last, cols]
            for j in range(last + 1):
                k = 8 * j + s
                total = total + taps_ref[k : k + 1, cols] * shifted[8 * j : 8 * j + out_rows]
        out_ref[:, cols] = total.astype(BF16)


def second_half(n_w, kind, info_ref, x_ref, *refs):
    w_refs, (c_ref, gain_ref, bias_ref, out_ref) = refs[:n_w], refs[n_w:]
    n_tp, rows, channels = c_ref.shape
    total_channels = n_tp * channels
    blocks = [c_ref[t].astype(F32) for t in range(n_tp)]
    mean = sum(jnp.sum(c, axis=1, keepdims=True) for c in blocks) / total_channels
    square = sum(jnp.sum(c * c, axis=1, keepdims=True) for c in blocks) / total_channels
    scale = lax.rsqrt(square - mean * mean + EPS)
    zs = w_refs[0].shape[1] // n_tp
    branch = jnp.zeros((rows, out_ref.shape[-1]), F32)
    for t in range(n_tp):
        cols = slice(t * channels, (t + 1) * channels)
        v = (blocks[t] - mean) * scale * gain_ref[:, cols] + bias_ref[:, cols]
        active = (v * jax.nn.sigmoid(v)).astype(BF16)
        w = weight_rows(w_refs, slice(t * zs, (t + 1) * zs), kind)
        part = lax.dot_general(active, w, (((1,), (1,)), ((), ())), preferred_element_type=F32)
        branch = branch + part.astype(BF16).astype(F32)
    out_ref[...] = (x_ref[RIM:].astype(F32) + turned(branch, info_ref[2])).astype(BF16)


def everyone(x, axis):
    blocks = jnp.broadcast_to(x[None], (lax.axis_size(axis), *x.shape))
    return lax.all_to_all(blocks, axis, 0, 0, tiled=True)


def round_y(x, step=None):
    ny, nc = lax.axis_size("y"), lax.axis_size("core")
    pairs = [(y * nc + c, (y + 1 - 2 * c) % ny * nc + c) for y in range(ny) for c in range(nc)]
    here = lax.all_gather(x, "core")
    parts, moving = [here], here
    for _ in range(ny // 2 - 1):
        moving = lax.ppermute(moving, ("y", "core"), pairs)
        parts.append(lax.all_gather(moving, "core"))
    half = lax.dynamic_index_in_dim(moving, lax.axis_index("core"), 0, keepdims=False)
    parts.append(lax.all_gather(lax.ppermute(half, ("y", "core"), pairs), "core"))
    return parts


def local(stream, norm_gain, value_weight, gate_weight, conv_taps, ln_gain, ln_bias, out_weight, final_gain):
    nz, ny, nc, nt = (lax.axis_size(a) for a in ("z", "y", "core", "tp"))
    tokens, columns = stream.shape
    channels = value_weight.shape[1]
    depth = value_weight.shape[0] // LAYERS
    tp, y = lax.axis_index("tp"), lax.axis_index("y")
    sp = (lax.axis_index("z") * ny + y) * nc + lax.axis_index("core")

    def per_layer(w):
        return jnp.moveaxis(w.reshape(depth, LAYERS, channels), 1, 0)

    count = nz * ny * nc
    halo = lax.ppermute(
        stream[-LAYERS * RIM :], ("z", "y", "core"), [(i, i + 1) for i in range(count - 1)]
    )
    zl = nz // nt
    pairs = [(z * nt + t, (t * zl + z % zl) * nt + z // zl) for z in range(nz) for t in range(nt)]
    out_t = lax.ppermute(per_layer(out_weight.T), ("z", "tp"), pairs)
    values, gates = per_layer(value_weight), per_layer(gate_weight)
    vg = jnp.stack([values[0], gates[0], values[1], gates[1]])
    vg_z = everyone(vg, "z")
    mine = jnp.concatenate([halo, stream], axis=0)
    x_all = [mine]
    for step in range(1, nt):
        x_all.append(lax.ppermute(mine, "tp", [(i, (i + step) % nt) for i in range(nt)]))
    vg_z, out_t = lax.optimization_barrier((vg_z, out_t))
    out_z = everyone(out_t, "z")
    out_z, *x_all = lax.optimization_barrier((out_z, *x_all))
    weights = [
        round_y(jnp.concatenate([vg_z[:, 2 * l : 2 * l + 2], out_z[:, l : l + 1]], axis=1))
        for l in range(LAYERS)
    ]

    my_taps = lax.dynamic_slice_in_dim(conv_taps, tp * channels, channels, 2)
    my_final = lax.dynamic_slice_in_dim(final_gain, tp * columns, columns, 0)
    wide = 2 * depth
    order = [(tp + nt - j) % nt for j in range(nt)]
    for layer in range(LAYERS):
        rows = tokens + (LAYERS - layer) * RIM
        out_rows = rows - RIM
        back = wide * y
        info = [jnp.where(sp == 0, rows - tokens, 0), jnp.where(y == 0, 0, wide * ny - back), back]
        info = jnp.stack(info + [jnp.int32(t) for t in order]).astype(jnp.int32)
        w = weights[layer]
        conv = call(
            lambda *refs: first_half(len(x_all), len(w), (0, 1), *refs),
            jax.ShapeDtypeStruct((out_rows, channels), BF16),
            len(x_all) + len(w) + 2,
            [pltpu.VMEM((rows, channels), F32)],
            flops=4 * rows * columns * nt * channels,
        )(info, *x_all, *w, norm_gain[layer].reshape(nt, 1, columns), my_taps[layer])
        conv = lax.all_gather(conv, "tp")
        mine = call(
            lambda *refs: second_half(len(w), 2, *refs),
            jax.ShapeDtypeStruct((out_rows, columns), BF16),
            len(w) + 4,
            flops=2 * out_rows * columns * nt * channels,
        )(info, mine, *w, conv, ln_gain[layer : layer + 1], ln_bias[layer : layer + 1])
        if layer < LAYERS - 1:
            x_all = [lax.all_gather(mine, "tp")]
            order = list(range(nt))
    final32 = mine.astype(F32)
    squares = lax.psum(jnp.sum(final32 * final32, axis=1), "tp")
    total = nt * columns
    return (final32 * lax.rsqrt(squares[:, None] / total + EPS) * my_final).astype(BF16)


def shape_of(mesh):
    n_sp, n_tp = mesh.devices.shape
    return n_sp // 16, 8, 2, n_tp


def solution(mesh):
    inner = Mesh(mesh.devices.reshape(shape_of(mesh)), ("z", "y", "core", "tp"))
    sp = ("z", "y", "core")
    placed = (P(sp, "tp"), P(), P(sp, "tp"), P(sp, "tp"), P(), P(), P(), P("tp", sp), P())
    return jax.shard_map(local, mesh=inner, in_specs=placed, out_specs=P(sp, "tp"), check_vma=False)
```

```python
import jax
import jax.numpy as jnp
from jax import lax
from jax.experimental import pallas as pl
from jax.experimental.pallas import tpu as pltpu
from jax.sharding import Mesh, PartitionSpec as P

KW = 31
LAYERS = 2
EPS = 1e-06
RIM = 32
LANES = 128
VMEM = pl.BlockSpec(memory_space=pltpu.VMEM)
SMEM = pl.BlockSpec(memory_space=pltpu.SMEM)
F32 = jnp.float32
BF16 = jnp.bfloat16
INTERPRET = False


def call(body, out_shape, n_in, scratch=(), flops=10**8):
    return pl.pallas_call(
        body,
        out_shape=out_shape,
        in_specs=[SMEM] + [VMEM] * n_in,
        out_specs=VMEM,
        scratch_shapes=list(scratch),
        cost_estimate=pl.CostEstimate(flops=flops, bytes_accessed=10**6, transcendentals=0),
        compiler_params=pltpu.CompilerParams(vmem_limit_bytes=20 * 2**20),
        interpret=INTERPRET,
    )


def weight_rows(refs, span, kind):
    here, *sides, far = refs
    ahead = [here] + [s.at[1] for s in sides] + [far] + [s.at[0] for s in reversed(sides)]
    blocks = [jnp.stack([b[core, span, kind] for core in range(2)], axis=1) for b in ahead]
    w = jnp.stack(blocks, axis=1)
    return w.reshape(-1, w.shape[-1])


def turned(x, shift):
    chunks = [
        pltpu.roll(x[:, low : low + LANES], shift, 1) for low in range(0, x.shape[1], LANES)
    ]
    return jnp.concatenate(chunks, axis=1)


def first_half(n_x, n_w, kinds, info_ref, *refs):
    x_refs, refs = refs[:n_x], refs[n_x:]
    w_refs, (gain_ref, taps_ref, out_ref, ext_ref) = refs[:n_w], refs[n_w:]
    n_tp, _, columns = gain_ref.shape
    rows, channels = ext_ref.shape
    zs = w_refs[0].shape[1] // n_tp
    copies, out_rows = out_ref.shape[:2]
    blocks = [(x_refs[t][...] if n_x > 1 else x_refs[0][t]).astype(F32) for t in range(n_tp)]
    squares = sum(jnp.sum(x * x, axis=1, keepdims=True) for x in blocks)
    scale = lax.rsqrt(squares / (n_tp * columns) + EPS)
    value = jnp.zeros((rows, channels), F32)
    gate = jnp.zeros((rows, channels), F32)
    for j in range(n_tp):
        t = info_ref[3 + j]
        normed = turned(blocks[j] * scale * gain_ref[t], info_ref[1]).astype(BF16)
        span = pl.ds(t * zs, zs)
        value = value + jnp.dot(normed, weight_rows(w_refs, span, kinds[0]), preferred_element_type=F32)
        gate = gate + jnp.dot(normed, weight_rows(w_refs, span, kinds[1]), preferred_element_type=F32)
    glu = value * jax.nn.sigmoid(gate)
    row = lax.broadcasted_iota(jnp.int32, glu.shape, 0)
    ext_ref[...] = jnp.where(row >= info_ref[0], glu, 0.0)
    lead = RIM - (KW - 1)
    lanes = min(channels, LANES)
    for low in range(0, channels, lanes):
        cols = slice(low, low + lanes)
        total = jnp.zeros((out_rows, lanes), F32)
        for s in range(8):
            last = (KW - 1 - s) // 8
            shifted = ext_ref[lead + s : lead + s + out_rows + 8 * last, cols]
            for j in range(last + 1):
                k = 8 * j + s
                total = total + taps_ref[k : k + 1, cols] * shifted[8 * j : 8 * j + out_rows]
        for copy in range(copies):
            out_ref[copy, :, cols] = total.astype(BF16)


def second_half(n_w, kind, info_ref, x_ref, *refs):
    w_refs, (c_ref, gain_ref, bias_ref, out_ref) = refs[:n_w], refs[n_w:]
    n_tp, rows, channels = c_ref.shape
    total_channels = n_tp * channels
    blocks = [c_ref[t].astype(F32) for t in range(n_tp)]
    mean = sum(jnp.sum(c, axis=1, keepdims=True) for c in blocks) / total_channels
    square = sum(jnp.sum(c * c, axis=1, keepdims=True) for c in blocks) / total_channels
    scale = lax.rsqrt(square - mean * mean + EPS)
    zs = w_refs[0].shape[1] // n_tp
    branch = jnp.zeros((rows, out_ref.shape[-1]), F32)
    for t in range(n_tp):
        cols = slice(t * channels, (t + 1) * channels)
        v = (blocks[t] - mean) * scale * gain_ref[:, cols] + bias_ref[:, cols]
        active = (v * jax.nn.sigmoid(v)).astype(BF16)
        w = weight_rows(w_refs, slice(t * zs, (t + 1) * zs), kind)
        part = lax.dot_general(active, w, (((1,), (1,)), ((), ())), preferred_element_type=F32)
        branch = branch + part.astype(BF16).astype(F32)
    x = x_ref[RIM:] if len(x_ref.shape) == 2 else x_ref[info_ref[3 + n_tp], RIM:]
    result = (x.astype(F32) + turned(branch, info_ref[2])).astype(BF16)
    for copy in range(out_ref.shape[0]):
        out_ref[copy] = result


def exchange(blocks, axis):
    return lax.all_to_all(blocks, axis, 0, 0, tiled=True)


def everyone(x, axis):
    return exchange(jnp.broadcast_to(x[None], (lax.axis_size(axis), *x.shape)), axis)


def round_y(x, step=None):
    ny, nc = lax.axis_size("y"), lax.axis_size("core")
    pairs = [(y * nc + c, (y + 1 - 2 * c) % ny * nc + c) for y in range(ny) for c in range(nc)]
    here = lax.all_gather(x, "core")
    parts, moving = [here], here
    for _ in range(ny // 2 - 1):
        moving = lax.ppermute(moving, ("y", "core"), pairs)
        parts.append(lax.all_gather(moving, "core"))
    half = lax.dynamic_index_in_dim(moving, lax.axis_index("core"), 0, keepdims=False)
    parts.append(lax.all_gather(lax.ppermute(half, ("y", "core"), pairs), "core"))
    return parts


def local(stream, norm_gain, value_weight, gate_weight, conv_taps, ln_gain, ln_bias, out_weight, final_gain):
    nz, ny, nc, nt = (lax.axis_size(a) for a in ("z", "y", "core", "tp"))
    tokens, columns = stream.shape
    channels = value_weight.shape[1]
    depth = value_weight.shape[0] // LAYERS
    tp, y = lax.axis_index("tp"), lax.axis_index("y")
    sp = (lax.axis_index("z") * ny + y) * nc + lax.axis_index("core")

    def per_layer(w):
        return jnp.moveaxis(w.reshape(depth, LAYERS, channels), 1, 0)

    count = nz * ny * nc
    halo = lax.ppermute(
        stream[-LAYERS * RIM :], ("z", "y", "core"), [(i, i + 1) for i in range(count - 1)]
    )
    zl = nz // nt
    pairs = [(z * nt + t, (t * zl + z % zl) * nt + z // zl) for z in range(nz) for t in range(nt)]
    out_t = lax.ppermute(per_layer(out_weight.T), ("z", "tp"), pairs)
    values, gates = per_layer(value_weight), per_layer(gate_weight)
    blocks = [w[l] for l in range(LAYERS) for w in (values, gates, out_t)]
    along_z = everyone(jnp.stack(blocks), "z")
    mine = jnp.concatenate([halo, stream], axis=0)
    x_all = [mine]
    for step in range(1, nt):
        x_all.append(lax.ppermute(mine, "tp", [(i, (i + step) % nt) for i in range(nt)]))
    along_z, *x_all = lax.optimization_barrier((along_z, *x_all))
    weights = [round_y(along_z[:, 3 * l : 3 * l + 3]) for l in range(LAYERS)]

    my_taps = lax.dynamic_slice_in_dim(conv_taps, tp * channels, channels, 2)
    my_final = lax.dynamic_slice_in_dim(final_gain, tp * columns, columns, 0)
    wide = 2 * depth
    order = [(tp + nt - j) % nt for j in range(nt)]
    for layer in range(LAYERS):
        rows = tokens + (LAYERS - layer) * RIM
        out_rows = rows - RIM
        back = wide * y
        info = [jnp.where(sp == 0, rows - tokens, 0), jnp.where(y == 0, 0, wide * ny - back), back]
        info = jnp.stack(info + [jnp.int32(t) for t in order] + [tp]).astype(jnp.int32)
        w = weights[layer]
        conv = call(
            lambda *refs: first_half(len(x_all), len(w), (0, 1), *refs),
            jax.ShapeDtypeStruct((nt, out_rows, channels), BF16),
            len(x_all) + len(w) + 2,
            [pltpu.VMEM((rows, channels), F32)],
            flops=4 * rows * columns * nt * channels,
        )(info, *x_all, *w, norm_gain[layer].reshape(nt, 1, columns), my_taps[layer])
        conv = exchange(conv, "tp")
        mine = call(
            lambda *refs: second_half(len(w), 2, *refs),
            jax.ShapeDtypeStruct((nt if layer < LAYERS - 1 else 1, out_rows, columns), BF16),
            len(w) + 4,
            flops=2 * out_rows * columns * nt * channels,
        )(info, mine, *w, conv, ln_gain[layer : layer + 1], ln_bias[layer : layer + 1])
        if layer < LAYERS - 1:
            mine = exchange(mine, "tp")
            x_all = [mine]
            order = list(range(nt))
    final32 = mine[0].astype(F32)
    squares = lax.psum(jnp.sum(final32 * final32, axis=1), "tp")
    total = nt * columns
    return (final32 * lax.rsqrt(squares[:, None] / total + EPS) * my_final).astype(BF16)


def shape_of(mesh):
    n_sp, n_tp = mesh.devices.shape
    return n_sp // 16, 8, 2, n_tp


def solution(mesh):
    inner = Mesh(mesh.devices.reshape(shape_of(mesh)), ("z", "y", "core", "tp"))
    sp = ("z", "y", "core")
    placed = (P(sp, "tp"), P(), P(sp, "tp"), P(sp, "tp"), P(), P(), P(), P("tp", sp), P())
    return jax.shard_map(local, mesh=inner, in_specs=placed, out_specs=P(sp, "tp"), check_vma=False)
```

```python
import functools

import jax
import jax.numpy as jnp
from jax import lax
from jax.experimental import pallas as pl
from jax.experimental.pallas import tpu as pltpu
from jax.sharding import Mesh, PartitionSpec as P

KW = 31
LAYERS = 2
EPS = 1e-06
RIM = 32
LANES = 128
VMEM = pl.BlockSpec(memory_space=pltpu.VMEM)
HBM = pl.BlockSpec(memory_space=pltpu.HBM)
F32 = jnp.float32
BF16 = jnp.bfloat16
INTERPRET = False


def call(body, out_shape, n_in, in_place, scratch, flops):
    return pl.pallas_call(
        body,
        out_shape=out_shape,
        in_specs=[HBM if i in in_place else VMEM for i in range(n_in)],
        out_specs=VMEM,
        scratch_shapes=[*scratch, pltpu.SemaphoreType.DMA((len(in_place),))],
        cost_estimate=pl.CostEstimate(flops=flops, bytes_accessed=10**6, transcendentals=0),
        compiler_params=pltpu.CompilerParams(vmem_limit_bytes=52 * 2**20),
        interpret=INTERPRET,
    )


def weight_rows(refs, span, kind):
    here, *sides, far = refs
    ahead = [here] + [s.at[1] for s in sides] + [far] + [s.at[0] for s in reversed(sides)]
    blocks = [jnp.stack([b[core, span, kind] for core in range(2)], axis=1) for b in ahead]
    w = jnp.stack(blocks, axis=1)
    return w.reshape(-1, w.shape[-1])


def turned(x, shift):
    chunks = [
        pltpu.roll(x[:, low : low + LANES], shift, 1) for low in range(0, x.shape[1], LANES)
    ]
    return jnp.concatenate(chunks, axis=1)


def position():
    y = lax.axis_index("y")
    first = (lax.axis_index("z") == 0) & (y == 0) & (lax.axis_index("core") == 0)
    return first, y, lax.axis_index("tp")


def fetch(refs, buffers, sems, low, count):
    copies = []
    for k, (ref, buf) in enumerate(zip(refs, buffers)):
        part = (slice(None),) * (len(ref.shape) - 3) + (pl.ds(low, count),)
        copies.append(pltpu.make_async_copy(ref.at[part], buf, sems.at[k]))
        copies[-1].start()
    return copies


def first_half(layer, n_w, *refs):
    w_hbm, (x_ref, gain_ref, taps_ref, out_ref, ext_ref, *w_refs, sems) = refs[:n_w], refs[n_w:]
    loads = fetch(w_hbm, w_refs, sems, 0, 2)
    n_tp, rows, columns = x_ref.shape
    channels = ext_ref.shape[1]
    zs = w_refs[0].shape[1] // n_tp
    copies, out_rows = out_ref.shape[:2]
    first, y, tp = position()
    lanes_y = LANES // lax.axis_size("y")
    blocks = [x_ref[t].astype(F32) for t in range(n_tp)]
    squares = sum(jnp.sum(x * x, axis=1, keepdims=True) for x in blocks)
    scale = lax.rsqrt(squares / (n_tp * columns) + EPS)
    value = jnp.zeros((rows, channels), F32)
    gate = jnp.zeros((rows, channels), F32)
    for load in loads:
        load.wait()
    for t in range(n_tp):
        gain = gain_ref[layer : layer + 1, t * columns : (t + 1) * columns]
        normed = turned(blocks[t] * scale * gain, (LANES - lanes_y * y) % LANES).astype(BF16)
        span = slice(t * zs, (t + 1) * zs)
        value = value + jnp.dot(normed, weight_rows(w_refs, span, 0), preferred_element_type=F32)
        gate = gate + jnp.dot(normed, weight_rows(w_refs, span, 1), preferred_element_type=F32)
    glu = value * jax.nn.sigmoid(gate)
    row = lax.broadcasted_iota(jnp.int32, glu.shape, 0)
    before = jnp.where(first, (LAYERS - layer) * RIM, 0)
    ext_ref[...] = jnp.where(row >= before, glu, 0.0)
    lead = RIM - (KW - 1)
    lanes = min(channels, LANES)
    for low in range(0, channels, lanes):
        cols = slice(low, low + lanes)
        mine = pl.ds(pl.multiple_of(tp * channels + low, lanes), lanes)
        taps = taps_ref[layer, :, mine]
        total = jnp.zeros((out_rows, lanes), F32)
        for s in range(8):
            last = (KW - 1 - s) // 8
            shifted = ext_ref[lead + s : lead + s + out_rows + 8 * last, cols]
            for j in range(last + 1):
                k = 8 * j + s
                total = total + taps[k : k + 1] * shifted[8 * j : 8 * j + out_rows]
        for copy in range(copies):
            out_ref[copy, :, cols] = total.astype(BF16)


def second_half(layer, n_w, *refs):
    w_hbm, (x_ref, c_ref, gain_ref, bias_ref, out_ref, x_buf, *w_refs, sems) = refs[:n_w], refs[n_w:]
    loads = fetch(w_hbm, w_refs, sems, 2, 1)
    first, y, tp = position()
    x_mine = x_ref if len(x_ref.shape) == 2 else x_ref.at[tp]
    loads.append(pltpu.make_async_copy(x_mine, x_buf, sems.at[n_w]))
    loads[-1].start()
    n_tp, rows, channels = c_ref.shape
    zs = w_refs[0].shape[1] // n_tp
    total_channels = n_tp * channels
    lanes_y = LANES // lax.axis_size("y")
    blocks = [c_ref[t].astype(F32) for t in range(n_tp)]
    mean = sum(jnp.sum(c, axis=1, keepdims=True) for c in blocks) / total_channels
    square = sum(jnp.sum(c * c, axis=1, keepdims=True) for c in blocks) / total_channels
    scale = lax.rsqrt(square - mean * mean + EPS)
    branch = jnp.zeros((rows, out_ref.shape[-1]), F32)
    for load in loads:
        load.wait()
    for t in range(n_tp):
        cols = slice(t * channels, (t + 1) * channels)
        gain, bias = gain_ref[layer : layer + 1, cols], bias_ref[layer : layer + 1, cols]
        v = (blocks[t] - mean) * scale * gain + bias
        active = (v * jax.nn.sigmoid(v)).astype(BF16)
        w = weight_rows(w_refs, slice(t * zs, (t + 1) * zs), 0)
        part = lax.dot_general(active, w, (((1,), (1,)), ((), ())), preferred_element_type=F32)
        branch = branch + part.astype(BF16).astype(F32)
    result = (x_buf[RIM:].astype(F32) + turned(branch, lanes_y * y)).astype(BF16)
    for copy in range(out_ref.shape[0]):
        out_ref[copy] = result


def exchange(blocks, axis):
    return lax.all_to_all(blocks, axis, 0, 0, tiled=True)


def everyone(x, axis):
    return exchange(jnp.broadcast_to(x[None], (lax.axis_size(axis), *x.shape)), axis)


def round_y(x, step=None):
    ny, nc = lax.axis_size("y"), lax.axis_size("core")
    pairs = [(y * nc + c, (y + 1 - 2 * c) % ny * nc + c) for y in range(ny) for c in range(nc)]
    here = lax.all_gather(x, "core")
    parts, moving = [here], here
    for _ in range(ny // 2 - 1):
        moving = lax.ppermute(moving, ("y", "core"), pairs)
        parts.append(lax.all_gather(moving, "core"))
    half = lax.dynamic_index_in_dim(moving, lax.axis_index("core"), 0, keepdims=False)
    parts.append(lax.all_gather(lax.ppermute(half, ("y", "core"), pairs), "core"))
    return parts


def local(stream, norm_gain, value_weight, gate_weight, conv_taps, ln_gain, ln_bias, out_weight, final_gain):
    nz, ny, nc, nt = (lax.axis_size(a) for a in ("z", "y", "core", "tp"))
    tokens, columns = stream.shape
    channels = value_weight.shape[1]
    depth = value_weight.shape[0] // LAYERS

    def per_layer(w):
        return jnp.moveaxis(w.reshape(depth, LAYERS, channels), 1, 0)

    count = nz * ny * nc
    halo = lax.ppermute(
        stream[-LAYERS * RIM :], ("z", "y", "core"), [(i, i + 1) for i in range(count - 1)]
    )
    zl = nz // nt
    pairs = [(z * nt + t, (t * zl + z % zl) * nt + z // zl) for z in range(nz) for t in range(nt)]
    out_t = lax.ppermute(per_layer(out_weight.T), ("z", "tp"), pairs)
    values, gates = per_layer(value_weight), per_layer(gate_weight)
    blocks = [w[l] for l in range(LAYERS) for w in (values, gates, out_t)]
    along_z = everyone(jnp.stack(blocks), "z")
    mine = jnp.concatenate([halo, stream], axis=0)
    x_all = lax.all_gather(mine, "tp")
    along_z, x_all = lax.optimization_barrier((along_z, x_all))
    weights = [round_y(along_z[:, 3 * l : 3 * l + 3]) for l in range(LAYERS)]

    for layer in range(LAYERS):
        rows = tokens + (LAYERS - layer) * RIM
        out_rows = rows - RIM
        w = weights[layer]

        def buffers(kinds):
            return [pltpu.VMEM((*p.shape[:-3], kinds, *p.shape[-2:]), BF16) for p in w]

        conv = call(
            functools.partial(first_half, layer, len(w)),
            jax.ShapeDtypeStruct((nt, out_rows, channels), BF16),
            len(w) + 3,
            range(len(w)),
            [pltpu.VMEM((rows, channels), F32), *buffers(2)],
            4 * rows * columns * nt * channels,
        )(*w, x_all, norm_gain, conv_taps)
        conv = exchange(conv, "tp")
        mine = call(
            functools.partial(second_half, layer, len(w)),
            jax.ShapeDtypeStruct((nt if layer < LAYERS - 1 else 1, out_rows, columns), BF16),
            len(w) + 4,
            range(len(w) + 1),
            [pltpu.VMEM((rows, columns), BF16), *buffers(1)],
            2 * out_rows * columns * nt * channels,
        )(*w, mine, conv, ln_gain, ln_bias)
        if layer < LAYERS - 1:
            x_all = mine = exchange(mine, "tp")
    final32 = mine[0].astype(F32)
    squares = jnp.sum(lax.all_gather(jnp.sum(final32 * final32, axis=1), "tp"), axis=0)
    my_final = lax.dynamic_slice_in_dim(final_gain, lax.axis_index("tp") * columns, columns, 0)
    return (final32 * lax.rsqrt(squares[:, None] / (nt * columns) + EPS) * my_final).astype(BF16)


def shape_of(mesh):
    n_sp, n_tp = mesh.devices.shape
    return n_sp // 16, 8, 2, n_tp


def solution(mesh):
    inner = Mesh(mesh.devices.reshape(shape_of(mesh)), ("z", "y", "core", "tp"))
    sp = ("z", "y", "core")
    placed = (P(sp, "tp"), P(), P(sp, "tp"), P(sp, "tp"), P(), P(), P(), P("tp", sp), P())
    return jax.shard_map(local, mesh=inner, in_specs=placed, out_specs=P(sp, "tp"), check_vma=False)
```

```python
import functools

import jax
import jax.numpy as jnp
from jax import lax
from jax.experimental import pallas as pl
from jax.experimental.pallas import tpu as pltpu
from jax.sharding import Mesh, PartitionSpec as P


KW = 31
LAYERS = 2
EPS = 1e-06
RIM = 32
LANES = 128
VMEM = pl.BlockSpec(memory_space=pltpu.VMEM)
HBM = pl.BlockSpec(memory_space=pltpu.HBM)
F32 = jnp.float32
BF16 = jnp.bfloat16
INTERPRET = False


def call(body, out_shape, n_in, in_place, copies, scratch, flops):
    return pl.pallas_call(
        body,
        out_shape=out_shape,
        in_specs=[HBM if i in in_place else VMEM for i in range(n_in)],
        out_specs=VMEM,
        scratch_shapes=[*scratch, pltpu.SemaphoreType.DMA((copies,))],
        cost_estimate=pl.CostEstimate(flops=flops, bytes_accessed=10**6, transcendentals=0),
        compiler_params=pltpu.CompilerParams(vmem_limit_bytes=52 * 2**20),
        interpret=INTERPRET,
    )


def weight_rows(refs, span, kind):
    here, *sides, far = refs
    ahead = [here] + [s.at[1] for s in sides] + [far] + [s.at[0] for s in reversed(sides)]
    blocks = [jnp.stack([b[core, span, kind] for core in range(2)], axis=1) for b in ahead]
    w = jnp.stack(blocks, axis=1)
    return w.reshape(-1, w.shape[-1])


def turned(x, shift):
    chunks = [
        pltpu.roll(x[:, low : low + LANES], shift, 1) for low in range(0, x.shape[1], LANES)
    ]
    return jnp.concatenate(chunks, axis=1)


def position():
    y = lax.axis_index("y")
    first = (lax.axis_index("z") == 0) & (y == 0) & (lax.axis_index("core") == 0)
    return first, y, lax.axis_index("tp")


def fetch(refs, buffers, sems, low, count):
    here_ref, own_ref, other_ref = refs
    here, *sides, far = buffers
    core = lax.axis_index("core")
    half = here.shape[1] // 2
    kinds = pl.ds(low, count)
    halves = []
    for h in range(2):
        zs = pl.ds(h * half, half)
        pairs = [(here_ref.at[:, zs, kinds], here.at[:, zs])]
        for ref, place in ((own_ref, core), (other_ref, 1 - core)):
            for k, side in enumerate(sides):
                pairs.append((ref.at[2 * k : 2 * k + 2, zs, kinds], side.at[place, :, zs]))
            pairs.append((ref.at[2 * len(sides), zs, kinds], far.at[place, zs]))
        copies = [pltpu.make_async_copy(*p, sems.at[len(pairs) * h + i]) for i, p in enumerate(pairs)]
        for copy in copies:
            copy.start()
        halves.append(copies)
    return halves


def first_half(layer, n_w, *refs):
    w_hbm, (x_ref, gain_ref, taps_ref, out_ref, ext_ref, *w_refs, sems) = refs[:n_w], refs[n_w:]
    loads = fetch(w_hbm, w_refs, sems, 0, 2)
    n_tp, rows, columns = x_ref.shape
    channels = ext_ref.shape[1]
    zs = w_refs[0].shape[1] // n_tp
    copies, out_rows = out_ref.shape[:2]
    first, y, tp = position()
    lanes_y = LANES // lax.axis_size("y")
    blocks = [x_ref[t].astype(F32) for t in range(n_tp)]
    squares = sum(jnp.sum(x * x, axis=1, keepdims=True) for x in blocks)
    scale = lax.rsqrt(squares / (n_tp * columns) + EPS)
    value = jnp.zeros((rows, channels), F32)
    gate = jnp.zeros((rows, channels), F32)
    for t in range(n_tp):
        if t % (n_tp // 2) == 0:
            for load in loads.pop(0):
                load.wait()
        gain = gain_ref[layer : layer + 1, t * columns : (t + 1) * columns]
        normed = turned(blocks[t] * scale * gain, (LANES - lanes_y * y) % LANES).astype(BF16)
        span = slice(t * zs, (t + 1) * zs)
        value = value + jnp.dot(normed, weight_rows(w_refs, span, 0), preferred_element_type=F32)
        gate = gate + jnp.dot(normed, weight_rows(w_refs, span, 1), preferred_element_type=F32)
    glu = value * jax.nn.sigmoid(gate)
    row = lax.broadcasted_iota(jnp.int32, glu.shape, 0)
    before = jnp.where(first, (LAYERS - layer) * RIM, 0)
    ext_ref[...] = jnp.where(row >= before, glu, 0.0)
    lead = RIM - (KW - 1)
    lanes = min(channels, LANES)
    for low in range(0, channels, lanes):
        cols = slice(low, low + lanes)
        mine = pl.ds(pl.multiple_of(tp * channels + low, lanes), lanes)
        taps = taps_ref[layer, :, mine]
        total = jnp.zeros((out_rows, lanes), F32)
        for s in range(8):
            last = (KW - 1 - s) // 8
            shifted = ext_ref[lead + s : lead + s + out_rows + 8 * last, cols]
            for j in range(last + 1):
                k = 8 * j + s
                total = total + taps[k : k + 1] * shifted[8 * j : 8 * j + out_rows]
        for copy in range(copies):
            out_ref[copy, :, cols] = total.astype(BF16)


def second_half(layer, n_w, *refs):
    w_hbm, (x_ref, c_ref, gain_ref, bias_ref, out_ref, x_buf, *w_refs, sems) = refs[:n_w], refs[n_w:]
    loads = fetch(w_hbm, w_refs, sems, 2, 1)
    _, y, tp = position()
    x_mine = x_ref if len(x_ref.shape) == 2 else x_ref.at[tp]
    load_x = pltpu.make_async_copy(x_mine, x_buf, sems.at[sems.shape[0] - 1])
    load_x.start()
    n_tp, rows, channels = c_ref.shape
    zs = w_refs[0].shape[1] // n_tp
    total_channels = n_tp * channels
    lanes_y = LANES // lax.axis_size("y")
    blocks = [c_ref[t].astype(F32) for t in range(n_tp)]
    mean = sum(jnp.sum(c, axis=1, keepdims=True) for c in blocks) / total_channels
    square = sum(jnp.sum(c * c, axis=1, keepdims=True) for c in blocks) / total_channels
    scale = lax.rsqrt(square - mean * mean + EPS)
    branch = jnp.zeros((rows, out_ref.shape[-1]), F32)
    for t in range(n_tp):
        if t % (n_tp // 2) == 0:
            for load in loads.pop(0):
                load.wait()
        cols = slice(t * channels, (t + 1) * channels)
        gain, bias = gain_ref[layer : layer + 1, cols], bias_ref[layer : layer + 1, cols]
        v = (blocks[t] - mean) * scale * gain + bias
        active = (v * jax.nn.sigmoid(v)).astype(BF16)
        w = weight_rows(w_refs, slice(t * zs, (t + 1) * zs), 0)
        part = lax.dot_general(active, w, (((1,), (1,)), ((), ())), preferred_element_type=F32)
        branch = branch + part.astype(BF16).astype(F32)
    load_x.wait()
    result = (x_buf[RIM:].astype(F32) + turned(branch, lanes_y * y)).astype(BF16)
    for copy in range(out_ref.shape[0]):
        out_ref[copy] = result


def exchange(blocks, axis):
    return lax.all_to_all(blocks, axis, 0, 0, tiled=True)


def everyone(x, axis):
    return exchange(jnp.broadcast_to(x[None], (lax.axis_size(axis), *x.shape)), axis)


def step_y(moving):
    ny, nc = lax.axis_size("y"), lax.axis_size("core")
    pairs = [(y * nc + c, (y + 1 - 2 * c) % ny * nc + c) for y in range(ny) for c in range(nc)]
    return lax.ppermute(moving, ("y", "core"), pairs)


def last_y(arrived, steps):
    arrived = list(arrived)
    for _ in range(steps):
        arrived.append(step_y(arrived[-1]))
    half = lax.dynamic_slice_in_dim(arrived[-1], lax.axis_index("core"), 1, 0)
    arrived.append(step_y(half))
    own = jnp.concatenate(arrived, axis=0)
    return own, lax.ppermute(own, "core", [(0, 1), (1, 0)])


def local(stream, norm_gain, value_weight, gate_weight, conv_taps, ln_gain, ln_bias, out_weight, final_gain):
    nz, ny, nc, nt = (lax.axis_size(a) for a in ("z", "y", "core", "tp"))
    tokens, columns = stream.shape
    channels = value_weight.shape[1]
    depth = value_weight.shape[0] // LAYERS

    def per_layer(w):
        return jnp.moveaxis(w.reshape(depth, LAYERS, channels), 1, 0)

    count = nz * ny * nc
    halo = lax.ppermute(
        stream[-LAYERS * RIM :], ("z", "y", "core"), [(i, i + 1) for i in range(count - 1)]
    )
    zl = nz // nt
    pairs = [(z * nt + t, (t * zl + z % zl) * nt + z // zl) for z in range(nz) for t in range(nt)]
    out_t = lax.ppermute(per_layer(out_weight.T), ("z", "tp"), pairs)
    values, gates = per_layer(value_weight), per_layer(gate_weight)
    blocks = [w[l] for l in range(LAYERS) for w in (values, gates, out_t)]
    mine = jnp.concatenate([halo, stream], axis=0)
    blocks, mine = lax.optimization_barrier((jnp.stack(blocks), mine))
    along_z = everyone(blocks, "z")
    x_all = lax.all_gather(mine, "tp")
    along_z, x_all = lax.optimization_barrier((along_z, x_all))
    heres = [lax.all_gather(along_z[:, 3 * l : 3 * l + 3], "core") for l in range(LAYERS)]
    full = ny // 2 - 1
    early = []
    for l in range(LAYERS):
        first = step_y(heres[l])
        early.append([first, step_y(first)])
    weights = [(heres[l], *last_y(early[l], full - 2)) for l in range(LAYERS)]

    for layer in range(LAYERS):
        rows = tokens + (LAYERS - layer) * RIM
        out_rows = rows - RIM
        w = weights[layer]

        def buffers(kinds):
            block = (2, nz, kinds, depth, channels)
            sides = [pltpu.VMEM((2, *block), BF16) for _ in range(ny // 2 - 1)]
            return [pltpu.VMEM(block, BF16), *sides, pltpu.VMEM(block, BF16)]

        loads = 2 * (ny + 1)

        conv = call(
            functools.partial(first_half, layer, len(w)),
            jax.ShapeDtypeStruct((nt, out_rows, channels), BF16),
            len(w) + 3,
            range(len(w)),
            loads,
            [pltpu.VMEM((rows, channels), F32), *buffers(2)],
            4 * rows * columns * nt * channels,
        )(*w, x_all, norm_gain, conv_taps)
        conv = exchange(conv, "tp")
        mine = call(
            functools.partial(second_half, layer, len(w)),
            jax.ShapeDtypeStruct((nt if layer < LAYERS - 1 else 1, out_rows, columns), BF16),
            len(w) + 4,
            range(len(w) + 1),
            loads + 1,
            [pltpu.VMEM((rows, columns), BF16), *buffers(1)],
            2 * out_rows * columns * nt * channels,
        )(*w, mine, conv, ln_gain, ln_bias)
        if layer < LAYERS - 1:
            x_all = mine = exchange(mine, "tp")
    final32 = mine[0].astype(F32)
    squares = jnp.sum(lax.all_gather(jnp.sum(final32 * final32, axis=1), "tp"), axis=0)
    my_final = lax.dynamic_slice_in_dim(final_gain, lax.axis_index("tp") * columns, columns, 0)
    return (final32 * lax.rsqrt(squares[:, None] / (nt * columns) + EPS) * my_final).astype(BF16)


def shape_of(mesh):
    n_sp, n_tp = mesh.devices.shape
    return n_sp // 16, 8, 2, n_tp


def solution(mesh):
    inner = Mesh(mesh.devices.reshape(shape_of(mesh)), ("z", "y", "core", "tp"))
    sp = ("z", "y", "core")
    placed = (P(sp, "tp"), P(), P(sp, "tp"), P(sp, "tp"), P(), P(), P(), P("tp", sp), P())

    return jax.shard_map(local, mesh=inner, in_specs=placed, out_specs=P(sp, "tp"), check_vma=False)
```

```python
import functools

import jax
import jax.numpy as jnp
from jax import lax
from jax.experimental import pallas as pl
from jax.experimental.pallas import tpu as pltpu
from jax.sharding import Mesh, PartitionSpec as P


KW = 31
LAYERS = 2
EPS = 1e-06
RIM = 32
LANES = 128
VMEM = pl.BlockSpec(memory_space=pltpu.VMEM)
HBM = pl.BlockSpec(memory_space=pltpu.HBM)
F32 = jnp.float32
BF16 = jnp.bfloat16
INTERPRET = False


def call(body, out_shape, n_in, in_place, copies, scratch, flops):
    return pl.pallas_call(
        body,
        out_shape=out_shape,
        in_specs=[HBM if i in in_place else VMEM for i in range(n_in)],
        out_specs=VMEM,
        scratch_shapes=[*scratch, pltpu.SemaphoreType.DMA((copies,))],
        cost_estimate=pl.CostEstimate(flops=flops, bytes_accessed=10**6, transcendentals=0),
        compiler_params=pltpu.CompilerParams(vmem_limit_bytes=52 * 2**20),
        interpret=INTERPRET,
    )


def weight_rows(refs, span, kind):
    here, *sides, far = refs
    ahead = [here] + [s.at[1] for s in sides] + [far] + [s.at[0] for s in reversed(sides)]
    blocks = [jnp.stack([b[core, kind, span] for core in range(2)], axis=1) for b in ahead]
    w = jnp.stack(blocks, axis=1)
    return w.reshape(-1, w.shape[-1])


def turned(x, shift):
    chunks = [
        pltpu.roll(x[:, low : low + LANES], shift, 1) for low in range(0, x.shape[1], LANES)
    ]
    return jnp.concatenate(chunks, axis=1)


def position():
    y = lax.axis_index("y")
    first = (lax.axis_index("z") == 0) & (y == 0) & (lax.axis_index("core") == 0)
    return first, y, lax.axis_index("tp")


def fetch(refs, buffers, sems, low, count):
    half = buffers[0].shape[-3] // 2
    halves = []
    for h in range(2):
        zs = pl.ds(h * half, half)
        copies = []
        for k, (ref, buf) in enumerate(zip(refs, buffers)):
            lead = (slice(None),) * (len(ref.shape) - 4)
            source, target = ref.at[(*lead, pl.ds(low, count), zs)], buf.at[(*lead, slice(None), zs)]
            copies.append(pltpu.make_async_copy(source, target, sems.at[len(refs) * h + k]))
            copies[-1].start()
        halves.append(copies)
    return halves


def first_half(layer, n_w, *refs):
    w_hbm, (x_ref, gain_ref, taps_ref, out_ref, ext_ref, *w_refs, sems) = refs[:n_w], refs[n_w:]
    loads = fetch(w_hbm, w_refs, sems, 0, 2)
    n_tp, rows, columns = x_ref.shape
    channels = ext_ref.shape[1]
    zs = w_refs[0].shape[2] // n_tp
    copies, out_rows = out_ref.shape[:2]
    first, y, tp = position()
    lanes_y = LANES // lax.axis_size("y")
    blocks = [x_ref[t].astype(F32) for t in range(n_tp)]
    squares = sum(jnp.sum(x * x, axis=1, keepdims=True) for x in blocks)
    scale = lax.rsqrt(squares / (n_tp * columns) + EPS)
    value = jnp.zeros((rows, channels), F32)
    gate = jnp.zeros((rows, channels), F32)
    for t in range(n_tp):
        if t % (n_tp // 2) == 0:
            for load in loads.pop(0):
                load.wait()
        gain = gain_ref[layer : layer + 1, t * columns : (t + 1) * columns]
        normed = turned(blocks[t] * scale * gain, (LANES - lanes_y * y) % LANES).astype(BF16)
        span = slice(t * zs, (t + 1) * zs)
        value = value + jnp.dot(normed, weight_rows(w_refs, span, 0), preferred_element_type=F32)
        gate = gate + jnp.dot(normed, weight_rows(w_refs, span, 1), preferred_element_type=F32)
    glu = value * jax.nn.sigmoid(gate)
    row = lax.broadcasted_iota(jnp.int32, glu.shape, 0)
    before = jnp.where(first, (LAYERS - layer) * RIM, 0)
    ext_ref[...] = jnp.where(row >= before, glu, 0.0)
    lead = RIM - (KW - 1)
    lanes = min(channels, LANES)
    for low in range(0, channels, lanes):
        cols = slice(low, low + lanes)
        mine = pl.ds(pl.multiple_of(tp * channels + low, lanes), lanes)
        total = jnp.zeros((out_rows, lanes), F32)
        for s in range(8):
            last = (KW - 1 - s) // 8
            shifted = ext_ref[lead + s : lead + s + out_rows + 8 * last, cols]
            for j in range(last + 1):
                k = 8 * j + s
                total = total + taps_ref[k, layer : layer + 1, mine] * shifted[8 * j : 8 * j + out_rows]
        for copy in range(copies):
            out_ref[copy, :, cols] = total.astype(BF16)


def second_half(layer, n_w, *refs):
    w_hbm, (x_ref, c_ref, gain_ref, bias_ref, out_ref, x_buf, *w_refs, sems) = refs[:n_w], refs[n_w:]
    loads = fetch(w_hbm, w_refs, sems, 2, 1)
    _, y, tp = position()
    x_mine = x_ref if len(x_ref.shape) == 2 else x_ref.at[tp]
    load_x = pltpu.make_async_copy(x_mine, x_buf, sems.at[sems.shape[0] - 1])
    load_x.start()
    n_tp, rows, channels = c_ref.shape
    zs = w_refs[0].shape[2] // n_tp
    total_channels = n_tp * channels
    lanes_y = LANES // lax.axis_size("y")
    blocks = [c_ref[t].astype(F32) for t in range(n_tp)]
    mean = sum(jnp.sum(c, axis=1, keepdims=True) for c in blocks) / total_channels
    square = sum(jnp.sum(c * c, axis=1, keepdims=True) for c in blocks) / total_channels
    scale = lax.rsqrt(square - mean * mean + EPS)
    branch = jnp.zeros((rows, out_ref.shape[-1]), F32)
    for t in range(n_tp):
        if t % (n_tp // 2) == 0:
            for load in loads.pop(0):
                load.wait()
        cols = slice(t * channels, (t + 1) * channels)
        gain, bias = gain_ref[layer : layer + 1, cols], bias_ref[layer : layer + 1, cols]
        v = (blocks[t] - mean) * scale * gain + bias
        active = (v * jax.nn.sigmoid(v)).astype(BF16)
        w = weight_rows(w_refs, slice(t * zs, (t + 1) * zs), 0)
        part = lax.dot_general(active, w, (((1,), (1,)), ((), ())), preferred_element_type=F32)
        branch = branch + part.astype(BF16).astype(F32)
    load_x.wait()
    result = (x_buf[RIM:].astype(F32) + turned(branch, lanes_y * y)).astype(BF16)
    for copy in range(out_ref.shape[0]):
        out_ref[copy] = result


def exchange(blocks, axis):
    return lax.all_to_all(blocks, axis, 0, 0, tiled=True)


def everyone(x, axis):
    return exchange(jnp.broadcast_to(x[None], (lax.axis_size(axis), *x.shape)), axis)


def step_y(moving):
    ny, nc = lax.axis_size("y"), lax.axis_size("core")
    pairs = [(y * nc + c, (y + 1 - 2 * c) % ny * nc + c) for y in range(ny) for c in range(nc)]
    return lax.ppermute(moving, ("y", "core"), pairs)


def join(x):
    return lax.all_gather(x, "core")


def ring_y(x):
    moving = join(x)
    parts = [moving]
    for _ in range(1, lax.axis_size("y") // 2):
        moving = step_y(moving)
        parts.append(join(moving))
    half = lax.dynamic_index_in_dim(moving, lax.axis_index("core"), 0, keepdims=False)
    half = step_y(half)
    return [*parts, join(half)]


def local(stream, norm_gain, value_weight, gate_weight, conv_taps, ln_gain, ln_bias, out_weight, final_gain):
    nz, ny, nc, nt = (lax.axis_size(a) for a in ("z", "y", "core", "tp"))
    tokens, columns = stream.shape
    channels = value_weight.shape[1]
    depth = value_weight.shape[0] // LAYERS

    def per_layer(w):
        return jnp.moveaxis(w.reshape(depth, LAYERS, channels), 1, 0)

    count = nz * ny * nc
    halo = lax.ppermute(
        stream[-LAYERS * RIM :], ("z", "y", "core"), [(i, i + 1) for i in range(count - 1)]
    )
    zl = nz // nt
    pairs = [(z * nt + t, (t * zl + z % zl) * nt + z // zl) for z in range(nz) for t in range(nt)]
    out_t = lax.ppermute(per_layer(out_weight.T), ("z", "tp"), pairs)
    values, gates = per_layer(value_weight), per_layer(gate_weight)
    blocks = [w[l] for l in range(LAYERS) for w in (values, gates, out_t)]
    mine = jnp.concatenate([halo, stream], axis=0)
    blocks, mine = lax.optimization_barrier((jnp.stack(blocks), mine))
    along_z = everyone(blocks, "z")
    x_all = lax.all_gather(mine, "tp")
    along_z, x_all = lax.optimization_barrier((along_z, x_all))
    by_matrix = jnp.swapaxes(along_z, 0, 1)
    weights = [ring_y(by_matrix[3 * l : 3 * l + 3]) for l in range(LAYERS)]

    for layer in range(LAYERS):
        rows = tokens + (LAYERS - layer) * RIM
        out_rows = rows - RIM
        w = weights[layer]

        def buffers(kinds):
            block = (2, kinds, nz, depth, channels)
            sides = [pltpu.VMEM((2, *block), BF16) for _ in range(ny // 2 - 1)]
            return [pltpu.VMEM(block, BF16), *sides, pltpu.VMEM(block, BF16)]

        loads = 2 * len(w)

        conv = call(
            functools.partial(first_half, layer, len(w)),
            jax.ShapeDtypeStruct((nt, out_rows, channels), BF16),
            len(w) + 3,
            range(len(w)),
            loads,
            [pltpu.VMEM((rows, channels), F32), *buffers(2)],
            4 * rows * columns * nt * channels,
        )(*w, x_all, norm_gain, jnp.swapaxes(conv_taps, 0, 1))
        conv = exchange(conv, "tp")
        mine = call(
            functools.partial(second_half, layer, len(w)),
            jax.ShapeDtypeStruct((nt if layer < LAYERS - 1 else 1, out_rows, columns), BF16),
            len(w) + 4,
            range(len(w) + 1),
            loads + 1,
            [pltpu.VMEM((rows, columns), BF16), *buffers(1)],
            2 * out_rows * columns * nt * channels,
        )(*w, mine, conv, ln_gain, ln_bias)
        if layer < LAYERS - 1:
            x_all = mine = exchange(mine, "tp")
    final32 = mine[0].astype(F32)
    squares = jnp.sum(lax.all_gather(jnp.sum(final32 * final32, axis=1), "tp"), axis=0)
    my_final = lax.dynamic_slice_in_dim(final_gain, lax.axis_index("tp") * columns, columns, 0)
    return (final32 * lax.rsqrt(squares[:, None] / (nt * columns) + EPS) * my_final).astype(BF16)


def shape_of(mesh):
    n_sp, n_tp = mesh.devices.shape
    return n_sp // 16, 8, 2, n_tp


def solution(mesh):
    inner = Mesh(mesh.devices.reshape(shape_of(mesh)), ("z", "y", "core", "tp"))
    sp = ("z", "y", "core")
    placed = (P(sp, "tp"), P(), P(sp, "tp"), P(sp, "tp"), P(), P(), P(), P("tp", sp), P())

    return jax.shard_map(local, mesh=inner, in_specs=placed, out_specs=P(sp, "tp"), check_vma=False)
```

```python
import functools

import jax
import jax.numpy as jnp
from jax import lax
from jax.experimental import pallas as pl
from jax.experimental.pallas import tpu as pltpu
from jax.sharding import Mesh, PartitionSpec as P


KW = 31
LAYERS = 2
EPS = 1e-06
RIM = 32
LANES = 128
VMEM = pl.BlockSpec(memory_space=pltpu.VMEM)
HBM = pl.BlockSpec(memory_space=pltpu.HBM)
F32 = jnp.float32
BF16 = jnp.bfloat16
INTERPRET = False


def call(body, out_shape, n_in, in_place, copies, scratch, flops):
    return pl.pallas_call(
        body,
        out_shape=out_shape,
        in_specs=[HBM if i in in_place else VMEM for i in range(n_in)],
        out_specs=VMEM,
        scratch_shapes=[*scratch, pltpu.SemaphoreType.DMA((copies,))],
        cost_estimate=pl.CostEstimate(flops=flops, bytes_accessed=10**6, transcendentals=0),
        compiler_params=pltpu.CompilerParams(vmem_limit_bytes=52 * 2**20),
        interpret=INTERPRET,
    )


def weight_rows(refs, span, kind):
    here, *sides, far = refs
    ahead = [here] + [s.at[1] for s in sides] + [far] + [s.at[0] for s in reversed(sides)]
    blocks = [jnp.stack([b[core, kind, span] for core in range(2)], axis=1) for b in ahead]
    w = jnp.stack(blocks, axis=1)
    return w.reshape(-1, w.shape[-1])


def turned(x, shift):
    chunks = [
        pltpu.roll(x[:, low : low + LANES], shift, 1) for low in range(0, x.shape[1], LANES)
    ]
    return jnp.concatenate(chunks, axis=1)


def position():
    y = lax.axis_index("y")
    first = (lax.axis_index("z") == 0) & (y == 0) & (lax.axis_index("core") == 0)
    return first, y, lax.axis_index("tp")


def fetch(refs, buffers, sems, low, count):
    half = buffers[0].shape[-3] // 2
    halves = []
    for h in range(2):
        zs = pl.ds(h * half, half)
        copies = []
        for k, (ref, buf) in enumerate(zip(refs, buffers)):
            lead = (slice(None),) * (len(ref.shape) - 4)
            source, target = ref.at[(*lead, pl.ds(low, count), zs)], buf.at[(*lead, slice(None), zs)]
            copies.append(pltpu.make_async_copy(source, target, sems.at[len(refs) * h + k]))
            copies[-1].start()
        halves.append(copies)
    return halves


def first_half(layer, n_w, *refs):
    w_hbm, (x_ref, taps_ref, gain_ref, out_ref, ext_ref, x_buf, taps_buf, *w_refs, sems) = (
        refs[:n_w],
        refs[n_w:],
    )
    tp = lax.axis_index("tp")
    channels = ext_ref.shape[1]
    mine = pl.ds(pl.multiple_of(tp * channels, LANES), channels)
    small = [
        pltpu.make_async_copy(x_ref, x_buf, sems.at[2 * n_w]),
        pltpu.make_async_copy(taps_ref.at[:, :, mine], taps_buf, sems.at[2 * n_w + 1]),
    ]
    for load in small:
        load.start()
    loads = fetch(w_hbm, w_refs, sems, 0, 2)
    n_tp, rows, columns = x_ref.shape
    zs = w_refs[0].shape[2] // n_tp
    copies, out_rows = out_ref.shape[:2]
    first, y, _ = position()
    lanes_y = LANES // lax.axis_size("y")
    small[0].wait()
    blocks = [x_buf[t].astype(F32) for t in range(n_tp)]
    squares = sum(jnp.sum(x * x, axis=1, keepdims=True) for x in blocks)
    scale = lax.rsqrt(squares / (n_tp * columns) + EPS)
    value = jnp.zeros((rows, channels), F32)
    gate = jnp.zeros((rows, channels), F32)
    for t in range(n_tp):
        if t % (n_tp // 2) == 0:
            for load in loads.pop(0):
                load.wait()
        gain = gain_ref[layer : layer + 1, t * columns : (t + 1) * columns]
        normed = turned(blocks[t] * scale * gain, (LANES - lanes_y * y) % LANES).astype(BF16)
        span = slice(t * zs, (t + 1) * zs)
        value = value + jnp.dot(normed, weight_rows(w_refs, span, 0), preferred_element_type=F32)
        gate = gate + jnp.dot(normed, weight_rows(w_refs, span, 1), preferred_element_type=F32)
    glu = value * jax.nn.sigmoid(gate)
    row = lax.broadcasted_iota(jnp.int32, glu.shape, 0)
    before = jnp.where(first, (LAYERS - layer) * RIM, 0)
    ext_ref[...] = jnp.where(row >= before, glu, 0.0)
    lead = RIM - (KW - 1)
    small[1].wait()
    lanes = min(channels, LANES)
    for low in range(0, channels, lanes):
        cols = slice(low, low + lanes)
        total = jnp.zeros((out_rows, lanes), F32)
        for s in range(8):
            last = (KW - 1 - s) // 8
            shifted = ext_ref[lead + s : lead + s + out_rows + 8 * last, cols]
            for j in range(last + 1):
                k = 8 * j + s
                total = total + taps_buf[k, layer : layer + 1, cols] * shifted[8 * j : 8 * j + out_rows]
        for copy in range(copies):
            out_ref[copy, :, cols] = total.astype(BF16)


def second_half(layer, n_w, *refs):
    w_hbm, (x_ref, c_ref, gain_ref, bias_ref, out_ref, x_buf, *w_refs, sems) = refs[:n_w], refs[n_w:]
    loads = fetch(w_hbm, w_refs, sems, 2, 1)
    _, y, tp = position()
    x_mine = x_ref if len(x_ref.shape) == 2 else x_ref.at[tp]
    load_x = pltpu.make_async_copy(x_mine, x_buf, sems.at[sems.shape[0] - 1])
    load_x.start()
    n_tp, rows, channels = c_ref.shape
    zs = w_refs[0].shape[2] // n_tp
    total_channels = n_tp * channels
    lanes_y = LANES // lax.axis_size("y")
    blocks = [c_ref[t].astype(F32) for t in range(n_tp)]
    mean = sum(jnp.sum(c, axis=1, keepdims=True) for c in blocks) / total_channels
    square = sum(jnp.sum(c * c, axis=1, keepdims=True) for c in blocks) / total_channels
    scale = lax.rsqrt(square - mean * mean + EPS)
    branch = jnp.zeros((rows, out_ref.shape[-1]), F32)
    for t in range(n_tp):
        if t % (n_tp // 2) == 0:
            for load in loads.pop(0):
                load.wait()
        cols = slice(t * channels, (t + 1) * channels)
        gain, bias = gain_ref[layer : layer + 1, cols], bias_ref[layer : layer + 1, cols]
        v = (blocks[t] - mean) * scale * gain + bias
        active = (v * jax.nn.sigmoid(v)).astype(BF16)
        w = weight_rows(w_refs, slice(t * zs, (t + 1) * zs), 0)
        part = lax.dot_general(active, w, (((1,), (1,)), ((), ())), preferred_element_type=F32)
        branch = branch + part.astype(BF16).astype(F32)
    load_x.wait()
    result = (x_buf[RIM:].astype(F32) + turned(branch, lanes_y * y)).astype(BF16)
    for copy in range(out_ref.shape[0]):
        out_ref[copy] = result


def exchange(blocks, axis):
    return lax.all_to_all(blocks, axis, 0, 0, tiled=True)


def everyone(x, axis):
    return exchange(jnp.broadcast_to(x[None], (lax.axis_size(axis), *x.shape)), axis)


def step_y(moving):
    ny, nc = lax.axis_size("y"), lax.axis_size("core")
    pairs = [(y * nc + c, (y + 1 - 2 * c) % ny * nc + c) for y in range(ny) for c in range(nc)]
    return lax.ppermute(moving, ("y", "core"), pairs)


def join(x):
    return lax.all_gather(x, "core")


def ring_y(x):
    moving = join(x)
    parts = [moving]
    for _ in range(1, lax.axis_size("y") // 2):
        moving = step_y(moving)
        parts.append(join(moving))
    half = lax.dynamic_index_in_dim(moving, lax.axis_index("core"), 0, keepdims=False)
    half = step_y(half)
    return [*parts, join(half)]


def local(stream, norm_gain, value_weight, gate_weight, conv_taps, ln_gain, ln_bias, out_weight, final_gain):
    nz, ny, nc, nt = (lax.axis_size(a) for a in ("z", "y", "core", "tp"))
    tokens, columns = stream.shape
    channels = value_weight.shape[1]
    depth = value_weight.shape[0] // LAYERS

    def per_layer(w):
        return jnp.moveaxis(w.reshape(depth, LAYERS, channels), 1, 0)

    count = nz * ny * nc
    halo = lax.ppermute(
        stream[-LAYERS * RIM :], ("z", "y", "core"), [(i, i + 1) for i in range(count - 1)]
    )
    zl = nz // nt
    pairs = [(z * nt + t, (t * zl + z % zl) * nt + z // zl) for z in range(nz) for t in range(nt)]
    out_t = lax.ppermute(per_layer(out_weight.T), ("z", "tp"), pairs)
    values, gates = per_layer(value_weight), per_layer(gate_weight)
    blocks = [w[l] for l in range(LAYERS) for w in (values, gates, out_t)]
    mine = jnp.concatenate([halo, stream], axis=0)
    blocks, mine = lax.optimization_barrier((jnp.stack(blocks), mine))
    along_z = everyone(blocks, "z")
    x_all = lax.all_gather(mine, "tp")
    along_z, x_all = lax.optimization_barrier((along_z, x_all))
    by_matrix = jnp.swapaxes(along_z, 0, 1)
    weights = [ring_y(by_matrix[3 * l : 3 * l + 3]) for l in range(LAYERS)]

    for layer in range(LAYERS):
        rows = tokens + (LAYERS - layer) * RIM
        out_rows = rows - RIM
        w = weights[layer]

        def buffers(kinds):
            block = (2, kinds, nz, depth, channels)
            sides = [pltpu.VMEM((2, *block), BF16) for _ in range(ny // 2 - 1)]
            return [pltpu.VMEM(block, BF16), *sides, pltpu.VMEM(block, BF16)]

        loads = 2 * len(w)

        conv = call(
            functools.partial(first_half, layer, len(w)),
            jax.ShapeDtypeStruct((nt, out_rows, channels), BF16),
            len(w) + 3,
            range(len(w) + 2),
            loads + 2,
            [
                pltpu.VMEM((rows, channels), F32),
                pltpu.VMEM((nt, rows, columns), BF16),
                pltpu.VMEM((KW, LAYERS, channels), F32),
                *buffers(2),
            ],
            4 * rows * columns * nt * channels,
        )(*w, x_all, jnp.swapaxes(conv_taps, 0, 1), norm_gain)
        conv = exchange(conv, "tp")
        mine = call(
            functools.partial(second_half, layer, len(w)),
            jax.ShapeDtypeStruct((nt if layer < LAYERS - 1 else 1, out_rows, columns), BF16),
            len(w) + 4,
            range(len(w) + 1),
            loads + 1,
            [pltpu.VMEM((rows, columns), BF16), *buffers(1)],
            2 * out_rows * columns * nt * channels,
        )(*w, mine, conv, ln_gain, ln_bias)
        if layer < LAYERS - 1:
            x_all = mine = exchange(mine, "tp")
    final32 = mine[0].astype(F32)
    squares = jnp.sum(lax.all_gather(jnp.sum(final32 * final32, axis=1), "tp"), axis=0)
    my_final = lax.dynamic_slice_in_dim(final_gain, lax.axis_index("tp") * columns, columns, 0)
    return (final32 * lax.rsqrt(squares[:, None] / (nt * columns) + EPS) * my_final).astype(BF16)


def shape_of(mesh):
    n_sp, n_tp = mesh.devices.shape
    return n_sp // 16, 8, 2, n_tp


def solution(mesh):
    inner = Mesh(mesh.devices.reshape(shape_of(mesh)), ("z", "y", "core", "tp"))
    sp = ("z", "y", "core")
    placed = (P(sp, "tp"), P(), P(sp, "tp"), P(sp, "tp"), P(), P(), P(), P("tp", sp), P())

    return jax.shard_map(local, mesh=inner, in_specs=placed, out_specs=P(sp, "tp"), check_vma=False)
```

```python
import functools

import jax
import jax.numpy as jnp
from jax import lax
from jax.experimental import pallas as pl
from jax.experimental.pallas import tpu as pltpu
from jax.sharding import Mesh, PartitionSpec as P


KW = 31
LAYERS = 2
EPS = 1e-06
RIM = 32
LANES = 128
VMEM = pl.BlockSpec(memory_space=pltpu.VMEM)
HBM = pl.BlockSpec(memory_space=pltpu.HBM)
F32 = jnp.float32
BF16 = jnp.bfloat16
INTERPRET = False


def call(body, out_shape, n_in, in_place, copies, scratch, flops):
    return pl.pallas_call(
        body,
        out_shape=out_shape,
        in_specs=[HBM if i in in_place else VMEM for i in range(n_in)],
        out_specs=VMEM,
        scratch_shapes=[*scratch, pltpu.SemaphoreType.DMA((copies,))],
        cost_estimate=pl.CostEstimate(flops=flops, bytes_accessed=10**6, transcendentals=0),
        compiler_params=pltpu.CompilerParams(vmem_limit_bytes=52 * 2**20),
        interpret=INTERPRET,
    )


def weight_rows(refs, span, kind):
    here, *sides, far = refs
    ahead = [here] + [s.at[1] for s in sides] + [far] + [s.at[0] for s in reversed(sides)]
    blocks = [jnp.stack([b[core, kind, span] for core in range(2)], axis=1) for b in ahead]
    w = jnp.stack(blocks, axis=1)
    return w.reshape(-1, w.shape[-1])


def turned(x, shift):
    chunks = [
        pltpu.roll(x[:, low : low + LANES], shift, 1) for low in range(0, x.shape[1], LANES)
    ]
    return jnp.concatenate(chunks, axis=1)


def position():
    y = lax.axis_index("y")
    first = (lax.axis_index("z") == 0) & (y == 0) & (lax.axis_index("core") == 0)
    return first, y, lax.axis_index("tp")


def fetch(refs, buffers, sems, low, count):
    half = buffers[0].shape[-3] // 2
    halves = []
    for h in range(2):
        zs = pl.ds(h * half, half)
        copies = []
        for k, (ref, buf) in enumerate(zip(refs, buffers)):
            lead = (slice(None),) * (len(ref.shape) - 4)
            source, target = ref.at[(*lead, pl.ds(low, count), zs)], buf.at[(*lead, slice(None), zs)]
            copies.append(pltpu.make_async_copy(source, target, sems.at[len(refs) * h + k]))
            copies[-1].start()
        halves.append(copies)
    return halves


def first_half(layer, n_w, *refs):
    w_hbm, (x_ref, taps_ref, gain_ref, out_ref, ext_ref, x_buf, taps_buf, *w_refs, sems) = (
        refs[:n_w],
        refs[n_w:],
    )
    tp = lax.axis_index("tp")
    channels = ext_ref.shape[1]
    mine = pl.ds(pl.multiple_of(tp * channels, LANES), channels)
    load_x = pltpu.make_async_copy(x_ref, x_buf, sems.at[2 * n_w])
    load_taps = pltpu.make_async_copy(taps_ref.at[:, :, mine], taps_buf, sems.at[2 * n_w + 1])
    if layer == 0:
        load_x.start()
    loads = fetch(w_hbm, w_refs, sems, 0, 2)
    load_taps.start()
    n_tp, rows, columns = x_ref.shape
    zs = w_refs[0].shape[2] // n_tp
    copies, out_rows = out_ref.shape[:2]
    first, y, _ = position()
    lanes_y = LANES // lax.axis_size("y")
    if layer == 0:
        load_x.wait()
    x_here = x_buf if layer == 0 else x_ref
    blocks = [x_here[t].astype(F32) for t in range(n_tp)]
    squares = sum(jnp.sum(x * x, axis=1, keepdims=True) for x in blocks)
    scale = lax.rsqrt(squares / (n_tp * columns) + EPS)
    value = jnp.zeros((rows, channels), F32)
    gate = jnp.zeros((rows, channels), F32)
    for t in range(n_tp):
        if t % (n_tp // 2) == 0:
            for load in loads.pop(0):
                load.wait()
        gain = gain_ref[layer : layer + 1, t * columns : (t + 1) * columns]
        normed = turned(blocks[t] * scale * gain, (LANES - lanes_y * y) % LANES).astype(BF16)
        span = slice(t * zs, (t + 1) * zs)
        value = value + jnp.dot(normed, weight_rows(w_refs, span, 0), preferred_element_type=F32)
        gate = gate + jnp.dot(normed, weight_rows(w_refs, span, 1), preferred_element_type=F32)
    glu = value * jax.nn.sigmoid(gate)
    row = lax.broadcasted_iota(jnp.int32, glu.shape, 0)
    before = jnp.where(first, (LAYERS - layer) * RIM, 0)
    ext_ref[...] = jnp.where(row >= before, glu, 0.0)
    lead = RIM - (KW - 1)
    load_taps.wait()
    lanes = min(channels, LANES)
    for low in range(0, channels, lanes):
        cols = slice(low, low + lanes)
        total = jnp.zeros((out_rows, lanes), F32)
        for s in range(8):
            last = (KW - 1 - s) // 8
            shifted = ext_ref[lead + s : lead + s + out_rows + 8 * last, cols]
            for j in range(last + 1):
                k = 8 * j + s
                total = total + taps_buf[k, layer : layer + 1, cols] * shifted[8 * j : 8 * j + out_rows]
        for copy in range(copies):
            out_ref[copy, :, cols] = total.astype(BF16)


def second_half(layer, n_w, *refs):
    w_hbm, (x_ref, c_ref, gain_ref, bias_ref, out_ref, x_buf, *w_refs, sems) = refs[:n_w], refs[n_w:]
    loads = fetch(w_hbm, w_refs, sems, 2, 1)
    _, y, tp = position()
    x_mine = x_ref if len(x_ref.shape) == 2 else x_ref.at[tp]
    load_x = pltpu.make_async_copy(x_mine, x_buf, sems.at[sems.shape[0] - 1])
    load_x.start()
    n_tp, rows, channels = c_ref.shape
    zs = w_refs[0].shape[2] // n_tp
    total_channels = n_tp * channels
    lanes_y = LANES // lax.axis_size("y")
    blocks = [c_ref[t].astype(F32) for t in range(n_tp)]
    mean = sum(jnp.sum(c, axis=1, keepdims=True) for c in blocks) / total_channels
    square = sum(jnp.sum(c * c, axis=1, keepdims=True) for c in blocks) / total_channels
    scale = lax.rsqrt(square - mean * mean + EPS)
    branch = jnp.zeros((rows, out_ref.shape[-1]), F32)
    for t in range(n_tp):
        if t % (n_tp // 2) == 0:
            for load in loads.pop(0):
                load.wait()
        cols = slice(t * channels, (t + 1) * channels)
        gain, bias = gain_ref[layer : layer + 1, cols], bias_ref[layer : layer + 1, cols]
        v = (blocks[t] - mean) * scale * gain + bias
        active = (v * jax.nn.sigmoid(v)).astype(BF16)
        w = weight_rows(w_refs, slice(t * zs, (t + 1) * zs), 0)
        part = lax.dot_general(active, w, (((1,), (1,)), ((), ())), preferred_element_type=F32)
        branch = branch + part.astype(BF16).astype(F32)
    load_x.wait()
    result = (x_buf[RIM:].astype(F32) + turned(branch, lanes_y * y)).astype(BF16)
    for copy in range(out_ref.shape[0]):
        out_ref[copy] = result


def exchange(blocks, axis):
    return lax.all_to_all(blocks, axis, 0, 0, tiled=True)


def everyone(x, axis):
    return exchange(jnp.broadcast_to(x[None], (lax.axis_size(axis), *x.shape)), axis)


def step_y(moving):
    ny, nc = lax.axis_size("y"), lax.axis_size("core")
    pairs = [(y * nc + c, (y + 1 - 2 * c) % ny * nc + c) for y in range(ny) for c in range(nc)]
    return lax.ppermute(moving, ("y", "core"), pairs)


def join(x):
    return lax.all_gather(x, "core")


def ring_y(x):
    moving = join(x)
    parts = [moving]
    for _ in range(1, lax.axis_size("y") // 2):
        moving = step_y(moving)
        parts.append(join(moving))
    half = lax.dynamic_index_in_dim(moving, lax.axis_index("core"), 0, keepdims=False)
    half = step_y(half)
    return [*parts, join(half)]


def local(stream, norm_gain, value_weight, gate_weight, conv_taps, ln_gain, ln_bias, out_weight, final_gain):
    nz, ny, nc, nt = (lax.axis_size(a) for a in ("z", "y", "core", "tp"))
    tokens, columns = stream.shape
    channels = value_weight.shape[1]
    depth = value_weight.shape[0] // LAYERS

    def per_layer(w):
        return jnp.moveaxis(w.reshape(depth, LAYERS, channels), 1, 0)

    count = nz * ny * nc
    halo = lax.ppermute(
        stream[-LAYERS * RIM :], ("z", "y", "core"), [(i, i + 1) for i in range(count - 1)]
    )
    zl = nz // nt
    pairs = [(z * nt + t, (t * zl + z % zl) * nt + z // zl) for z in range(nz) for t in range(nt)]
    out_t = lax.ppermute(per_layer(out_weight.T), ("z", "tp"), pairs)
    values, gates = per_layer(value_weight), per_layer(gate_weight)
    blocks = [w[l] for l in range(LAYERS) for w in (values, gates, out_t)]
    mine = jnp.concatenate([halo, stream], axis=0)
    blocks, mine = lax.optimization_barrier((jnp.stack(blocks), mine))
    along_z = everyone(blocks, "z")
    x_all = lax.all_gather(mine, "tp")
    along_z, x_all = lax.optimization_barrier((along_z, x_all))
    by_matrix = jnp.swapaxes(along_z, 0, 1)
    weights = [ring_y(by_matrix[3 * l : 3 * l + 3]) for l in range(LAYERS)]

    for layer in range(LAYERS):
        rows = tokens + (LAYERS - layer) * RIM
        out_rows = rows - RIM
        w = weights[layer]

        def buffers(kinds):
            block = (2, kinds, nz, depth, channels)
            sides = [pltpu.VMEM((2, *block), BF16) for _ in range(ny // 2 - 1)]
            return [pltpu.VMEM(block, BF16), *sides, pltpu.VMEM(block, BF16)]

        loads = 2 * len(w)

        conv = call(
            functools.partial(first_half, layer, len(w)),
            jax.ShapeDtypeStruct((nt, out_rows, channels), BF16),
            len(w) + 3,
            [i for i in range(len(w) + 2) if layer == 0 or i != len(w)],
            loads + 2,
            [
                pltpu.VMEM((rows, channels), F32),
                pltpu.VMEM((nt, rows, columns), BF16),
                pltpu.VMEM((KW, LAYERS, channels), F32),
                *buffers(2),
            ],
            4 * rows * columns * nt * channels,
        )(*w, x_all, jnp.swapaxes(conv_taps, 0, 1), norm_gain)
        conv = exchange(conv, "tp")
        mine = call(
            functools.partial(second_half, layer, len(w)),
            jax.ShapeDtypeStruct((nt if layer < LAYERS - 1 else 1, out_rows, columns), BF16),
            len(w) + 4,
            range(len(w) + 1),
            loads + 1,
            [pltpu.VMEM((rows, columns), BF16), *buffers(1)],
            2 * out_rows * columns * nt * channels,
        )(*w, mine, conv, ln_gain, ln_bias)
        if layer < LAYERS - 1:
            x_all = mine = exchange(mine, "tp")
    final32 = mine[0].astype(F32)
    squares = jnp.sum(lax.all_gather(jnp.sum(final32 * final32, axis=1), "tp"), axis=0)
    my_final = lax.dynamic_slice_in_dim(final_gain, lax.axis_index("tp") * columns, columns, 0)
    return (final32 * lax.rsqrt(squares[:, None] / (nt * columns) + EPS) * my_final).astype(BF16)


def shape_of(mesh):
    n_sp, n_tp = mesh.devices.shape
    return n_sp // 16, 8, 2, n_tp


def solution(mesh):
    inner = Mesh(mesh.devices.reshape(shape_of(mesh)), ("z", "y", "core", "tp"))
    sp = ("z", "y", "core")
    placed = (P(sp, "tp"), P(), P(sp, "tp"), P(sp, "tp"), P(), P(), P(), P("tp", sp), P())

    return jax.shard_map(local, mesh=inner, in_specs=placed, out_specs=P(sp, "tp"), check_vma=False)
```

```python
import functools

import jax
import jax.numpy as jnp
from jax import lax
from jax.experimental import pallas as pl
from jax.experimental.pallas import tpu as pltpu
from jax.sharding import Mesh, PartitionSpec as P


KW = 31
LAYERS = 2
EPS = 1e-06
RIM = 32
LANES = 128
VMEM = pl.BlockSpec(memory_space=pltpu.VMEM)
HBM = pl.BlockSpec(memory_space=pltpu.HBM)
F32 = jnp.float32
BF16 = jnp.bfloat16
INTERPRET = False


def call(body, out_shape, n_in, in_place, copies, scratch, flops):
    return pl.pallas_call(
        body,
        out_shape=out_shape,
        in_specs=[HBM if i in in_place else VMEM for i in range(n_in)],
        out_specs=VMEM,
        scratch_shapes=[*scratch, pltpu.SemaphoreType.DMA((copies,))],
        cost_estimate=pl.CostEstimate(flops=flops, bytes_accessed=10**6, transcendentals=0),
        compiler_params=pltpu.CompilerParams(vmem_limit_bytes=52 * 2**20),
        interpret=INTERPRET,
    )


def weight_rows(refs, span, kind):
    here, *sides, far = refs
    ahead = [here] + [s.at[1] for s in sides] + [far] + [s.at[0] for s in reversed(sides)]
    blocks = [jnp.stack([b[core, kind, span] for core in range(2)], axis=1) for b in ahead]
    w = jnp.stack(blocks, axis=1)
    return w.reshape(-1, w.shape[-1])


def turned(x, shift):
    chunks = [
        pltpu.roll(x[:, low : low + LANES], shift, 1) for low in range(0, x.shape[1], LANES)
    ]
    return jnp.concatenate(chunks, axis=1)


def position():
    y = lax.axis_index("y")
    first = (lax.axis_index("z") == 0) & (y == 0) & (lax.axis_index("core") == 0)
    return first, y, lax.axis_index("tp")


def fetch(refs, buffers, sems, low, count):
    n_tp = lax.axis_size("tp")
    width = buffers[0].shape[-3] // n_tp
    blocks = []
    for h in range(n_tp):
        zs = pl.ds(h * width, width)
        copies = []
        for k, (ref, buf) in enumerate(zip(refs, buffers)):
            lead = (slice(None),) * (len(ref.shape) - 4)
            source, target = ref.at[(*lead, pl.ds(low, count), zs)], buf.at[(*lead, slice(None), zs)]
            copies.append(pltpu.make_async_copy(source, target, sems.at[len(refs) * h + k]))
            copies[-1].start()
        blocks.append(copies)
    return blocks


def first_half(layer, n_w, *refs):
    w_hbm, (x_ref, taps_ref, gain_ref, out_ref, ext_ref, x_buf, taps_buf, *w_refs, sems) = (
        refs[:n_w],
        refs[n_w:],
    )
    tp = lax.axis_index("tp")
    channels = ext_ref.shape[1]
    mine = pl.ds(pl.multiple_of(tp * channels, LANES), channels)
    load_x = pltpu.make_async_copy(x_ref, x_buf, sems.at[sems.shape[0] - 1])
    load_taps = pltpu.make_async_copy(taps_ref.at[:, :, mine], taps_buf, sems.at[sems.shape[0] - 2])
    if layer == 0:
        load_x.start()
    loads = fetch(w_hbm, w_refs, sems, 0, 2)
    load_taps.start()
    n_tp, rows, columns = x_ref.shape
    zs = w_refs[0].shape[2] // n_tp
    copies, out_rows = out_ref.shape[:2]
    first, y, _ = position()
    lanes_y = LANES // lax.axis_size("y")
    if layer == 0:
        load_x.wait()
    x_here = x_buf if layer == 0 else x_ref
    blocks = [x_here[t].astype(F32) for t in range(n_tp)]
    squares = sum(jnp.sum(x * x, axis=1, keepdims=True) for x in blocks)
    scale = lax.rsqrt(squares / (n_tp * columns) + EPS)
    value = jnp.zeros((rows, channels), F32)
    gate = jnp.zeros((rows, channels), F32)
    for t in range(n_tp):
        for load in loads[t]:
            load.wait()
        gain = gain_ref[layer : layer + 1, t * columns : (t + 1) * columns]
        normed = turned(blocks[t] * scale * gain, (LANES - lanes_y * y) % LANES).astype(BF16)
        span = slice(t * zs, (t + 1) * zs)
        value = value + jnp.dot(normed, weight_rows(w_refs, span, 0), preferred_element_type=F32)
        gate = gate + jnp.dot(normed, weight_rows(w_refs, span, 1), preferred_element_type=F32)
    glu = value * jax.nn.sigmoid(gate)
    row = lax.broadcasted_iota(jnp.int32, glu.shape, 0)
    before = jnp.where(first, (LAYERS - layer) * RIM, 0)
    ext_ref[...] = jnp.where(row >= before, glu, 0.0)
    lead = RIM - (KW - 1)
    load_taps.wait()
    lanes = min(channels, LANES)
    for low in range(0, channels, lanes):
        cols = slice(low, low + lanes)
        total = jnp.zeros((out_rows, lanes), F32)
        for s in range(8):
            last = (KW - 1 - s) // 8
            shifted = ext_ref[lead + s : lead + s + out_rows + 8 * last, cols]
            for j in range(last + 1):
                k = 8 * j + s
                total = total + taps_buf[k, layer : layer + 1, cols] * shifted[8 * j : 8 * j + out_rows]
        for copy in range(copies):
            out_ref[copy, :, cols] = total.astype(BF16)


def second_half(layer, n_w, *refs):
    w_hbm, (x_ref, c_ref, gain_ref, bias_ref, out_ref, x_buf, *w_refs, sems) = refs[:n_w], refs[n_w:]
    loads = fetch(w_hbm, w_refs, sems, 2, 1)
    _, y, tp = position()
    x_mine = x_ref if len(x_ref.shape) == 2 else x_ref.at[tp]
    load_x = pltpu.make_async_copy(x_mine, x_buf, sems.at[sems.shape[0] - 1])
    load_x.start()
    n_tp, rows, channels = c_ref.shape
    zs = w_refs[0].shape[2] // n_tp
    total_channels = n_tp * channels
    lanes_y = LANES // lax.axis_size("y")
    blocks = [c_ref[t].astype(F32) for t in range(n_tp)]
    mean = sum(jnp.sum(c, axis=1, keepdims=True) for c in blocks) / total_channels
    square = sum(jnp.sum(c * c, axis=1, keepdims=True) for c in blocks) / total_channels
    scale = lax.rsqrt(square - mean * mean + EPS)
    branch = jnp.zeros((rows, out_ref.shape[-1]), F32)
    for t in range(n_tp):
        for load in loads[t]:
            load.wait()
        cols = slice(t * channels, (t + 1) * channels)
        gain, bias = gain_ref[layer : layer + 1, cols], bias_ref[layer : layer + 1, cols]
        v = (blocks[t] - mean) * scale * gain + bias
        active = (v * jax.nn.sigmoid(v)).astype(BF16)
        w = weight_rows(w_refs, slice(t * zs, (t + 1) * zs), 0)
        part = lax.dot_general(active, w, (((1,), (1,)), ((), ())), preferred_element_type=F32)
        branch = branch + part.astype(BF16).astype(F32)
    load_x.wait()
    result = (x_buf[RIM:].astype(F32) + turned(branch, lanes_y * y)).astype(BF16)
    for copy in range(out_ref.shape[0]):
        out_ref[copy] = result


def exchange(blocks, axis):
    return lax.all_to_all(blocks, axis, 0, 0, tiled=True)


def everyone(x, axis):
    return exchange(jnp.broadcast_to(x[None], (lax.axis_size(axis), *x.shape)), axis)


def step_y(moving):
    ny, nc = lax.axis_size("y"), lax.axis_size("core")
    pairs = [(y * nc + c, (y + 1 - 2 * c) % ny * nc + c) for y in range(ny) for c in range(nc)]
    return lax.ppermute(moving, ("y", "core"), pairs)


def join(x):
    return lax.all_gather(x, "core")


def ring_y(x):
    moving = join(x)
    parts = [moving]
    for _ in range(1, lax.axis_size("y") // 2):
        moving = step_y(moving)
        parts.append(join(moving))
    half = lax.dynamic_index_in_dim(moving, lax.axis_index("core"), 0, keepdims=False)
    half = step_y(half)
    return [*parts, join(half)]


def local(stream, norm_gain, value_weight, gate_weight, conv_taps, ln_gain, ln_bias, out_weight, final_gain):
    nz, ny, nc, nt = (lax.axis_size(a) for a in ("z", "y", "core", "tp"))
    tokens, columns = stream.shape
    channels = value_weight.shape[1]
    depth = value_weight.shape[0] // LAYERS

    def per_layer(w):
        return jnp.moveaxis(w.reshape(depth, LAYERS, channels), 1, 0)

    count = nz * ny * nc
    halo = lax.ppermute(
        stream[-LAYERS * RIM :], ("z", "y", "core"), [(i, i + 1) for i in range(count - 1)]
    )
    zl = nz // nt
    pairs = [(z * nt + t, (t * zl + z % zl) * nt + z // zl) for z in range(nz) for t in range(nt)]
    out_t = lax.ppermute(per_layer(out_weight.T), ("z", "tp"), pairs)
    values, gates = per_layer(value_weight), per_layer(gate_weight)
    blocks = [w[l] for l in range(LAYERS) for w in (values, gates, out_t)]
    mine = jnp.concatenate([halo, stream], axis=0)
    blocks, mine = lax.optimization_barrier((jnp.stack(blocks), mine))
    along_z = everyone(blocks, "z")
    x_all = lax.all_gather(mine, "tp")
    along_z, x_all = lax.optimization_barrier((along_z, x_all))
    by_matrix = jnp.swapaxes(along_z, 0, 1)
    weights = [ring_y(by_matrix[3 * l : 3 * l + 3]) for l in range(LAYERS)]

    for layer in range(LAYERS):
        rows = tokens + (LAYERS - layer) * RIM
        out_rows = rows - RIM
        w = weights[layer]

        def buffers(kinds):
            block = (2, kinds, nz, depth, channels)
            sides = [pltpu.VMEM((2, *block), BF16) for _ in range(ny // 2 - 1)]
            return [pltpu.VMEM(block, BF16), *sides, pltpu.VMEM(block, BF16)]

        loads = nt * len(w)

        conv = call(
            functools.partial(first_half, layer, len(w)),
            jax.ShapeDtypeStruct((nt, out_rows, channels), BF16),
            len(w) + 3,
            [i for i in range(len(w) + 2) if layer == 0 or i != len(w)],
            loads + 2,
            [
                pltpu.VMEM((rows, channels), F32),
                pltpu.VMEM((nt, rows, columns), BF16),
                pltpu.VMEM((KW, LAYERS, channels), F32),
                *buffers(2),
            ],
            4 * rows * columns * nt * channels,
        )(*w, x_all, jnp.swapaxes(conv_taps, 0, 1), norm_gain)
        conv = exchange(conv, "tp")
        mine = call(
            functools.partial(second_half, layer, len(w)),
            jax.ShapeDtypeStruct((nt if layer < LAYERS - 1 else 1, out_rows, columns), BF16),
            len(w) + 4,
            range(len(w) + 1),
            loads + 1,
            [pltpu.VMEM((rows, columns), BF16), *buffers(1)],
            2 * out_rows * columns * nt * channels,
        )(*w, mine, conv, ln_gain, ln_bias)
        if layer < LAYERS - 1:
            x_all = mine = exchange(mine, "tp")
    final32 = mine[0].astype(F32)
    squares = jnp.sum(lax.all_gather(jnp.sum(final32 * final32, axis=1), "tp"), axis=0)
    my_final = lax.dynamic_slice_in_dim(final_gain, lax.axis_index("tp") * columns, columns, 0)
    return (final32 * lax.rsqrt(squares[:, None] / (nt * columns) + EPS) * my_final).astype(BF16)


def shape_of(mesh):
    n_sp, n_tp = mesh.devices.shape
    return n_sp // 16, 8, 2, n_tp


def solution(mesh):
    inner = Mesh(mesh.devices.reshape(shape_of(mesh)), ("z", "y", "core", "tp"))
    sp = ("z", "y", "core")
    placed = (P(sp, "tp"), P(), P(sp, "tp"), P(sp, "tp"), P(), P(), P(), P("tp", sp), P())

    return jax.shard_map(local, mesh=inner, in_specs=placed, out_specs=P(sp, "tp"), check_vma=False)
```
